32 devices in a mesh: sp: 16 (over z, y, core), tp: 2 (over x).
Axes of the slice: x: 2, y: 2, z: 4, core: 2. Of those that a mesh axis runs over, the one named last changes fastest.
Arguments:
- query_rows: bfloat16 [8192, 1024], P(('sp', 'tp')), may hold values from -6 to 6
- key_rows: bfloat16 [8192, 1024], P(('sp', 'tp')), may hold values from -6 to 6
- value_rows: bfloat16 [8192, 1024], P(('sp', 'tp')), may hold values from -6 to 6
- out_grad: bfloat16 [8192, 1024], P(('sp', 'tp')), may hold values from -40 to 40
- log_totals: float32 [8192, 8], P(('sp', 'tp')), may hold values from 6 to 7.5
- out_dot: float32 [8192, 8], P(('sp', 'tp')), may hold values from -6 to 6
- bias_table: float32 [8, 320], replicated, may hold values from -4 to 4
Outputs:
- grad_query: bfloat16 [8192, 1024], P(('sp', 'tp'))
- grad_key: bfloat16 [8192, 1024], P(('sp', 'tp'))
- grad_value: bfloat16 [8192, 1024], P(('sp', 'tp'))
- grad_table: float32 [8, 320], replicated
The draws below stay inside these ranges and needn't reach their ends.
All inputs are finite; a program needn't handle non-finite values.
Results may differ from the reference program's by a relative error of at most 0.005.
Values may be sent and summed in bfloat16 or wider, within the bound.
A program may use at most 128 MiB of HBM per device.

```python
import jax
import jax.numpy as jnp
from jax import lax

HEADS = 8
HEAD_DIM = 128
SEG_LEN = 64
LEFT_SEGS = 8
REL_CLIP = 256
TOK_DEV = 256
MIX_WIDTH = 1024
TABLE_LEN = 320
BACK_DEVS = 2
TOKENS = 8192


def draw_out_grad(key, part):
    position = jnp.arange(TOKENS, dtype=jnp.float32) / TOKENS
    base_vals = jnp.clip(jax.random.normal(key, (TOKENS, HEADS * HEAD_DIM), jnp.float32), -6.0, 6.0)
    growth = 3.0 ** position
    return (base_vals * growth[:, None]).astype(jnp.bfloat16)


def block_levels(rng, shape, shards, low, largest):
    loudness, own = 1.0, jax.random.fold_in(rng, 6)
    for axis_at, shards_of in shards:
        heights = jnp.exp(jax.random.uniform(jax.random.fold_in(own, axis_at), (shards_of,), jnp.float32, low / len(shards), largest / len(shards)))
        loudness = loudness * jnp.repeat(heights, shape[axis_at] // shards_of).reshape([-1 if axis == axis_at else 1 for axis in range(len(shape))])
    return loudness


def noise(key, shape, deviation, bound, cuts=(), held_as=jnp.bfloat16):
    entries = jax.random.normal(key, shape, jnp.float32) * deviation
    if len(cuts) > 0:
        entries = block_levels(key, shape, cuts, -0.22, 0.18) * entries
    return jnp.clip(entries, min=-bound, max=bound).astype(held_as)


def setup_inputs(seed: int = 0) -> dict:
    key_of = jax.random.split(jax.random.key(seed), 8)
    query_rows = noise(key_of[0], (TOKENS, MIX_WIDTH), 1.0, 6.0, ((0, 32),))
    key_rows = noise(key_of[1], (TOKENS, MIX_WIDTH), 1.0, 6.0, ((0, 32),))
    value_rows = noise(key_of[2], (TOKENS, MIX_WIDTH), 1.0, 6.0, ((0, 32),))
    out_grad = draw_out_grad(jax.random.fold_in(key_of[7], 71), 0)
    log_totals = jnp.clip(6.0 + 1.5 * jax.random.uniform(key_of[4], (TOKENS, HEADS), jnp.float32) ** block_levels(key_of[4], (TOKENS, HEADS), ((0, 32),), -0.2, 0.2), 6.0, 7.5)
    out_dot = noise(key_of[5], (TOKENS, HEADS), 1.5, 6.0, ((0, 32),), jnp.float32)
    bias_table = noise(key_of[6], (HEADS, TABLE_LEN), 1.0, 4.0, (), jnp.float32)
    return dict(query_rows=query_rows, key_rows=key_rows, value_rows=value_rows, out_grad=out_grad, log_totals=log_totals, out_dot=out_dot, bias_table=bias_table)


def reference(query_rows, key_rows, value_rows, out_grad, log_totals, out_dot, bias_table):
    token_count = query_rows.shape[0]
    feature_count = query_rows.shape[1]
    head_count = bias_table.shape[0]
    head_size = feature_count // head_count
    block_rows = TOK_DEV
    lag_rows = BACK_DEVS * TOK_DEV
    window = lag_rows + block_rows
    inv_root = head_size ** -0.5
    padded_keys = jnp.concatenate([jnp.zeros((lag_rows, feature_count), query_rows.dtype), key_rows], axis=0)
    padded_values = jnp.concatenate([jnp.zeros((lag_rows, feature_count), query_rows.dtype), value_rows], axis=0)
    local_query = jnp.arange(block_rows, dtype=jnp.int32)
    local_key = jnp.arange(window, dtype=jnp.int32)
    distance = local_query[:, None] - local_key[None, :] + lag_rows
    table_index = (jnp.clip(distance, 1 - SEG_LEN, REL_CLIP) + SEG_LEN - 1).astype(jnp.int32)
    bias_vals = bias_table[:, table_index]
    seg_gap = (local_query[:, None] + lag_rows) // SEG_LEN - (local_key // SEG_LEN)[None, :]
    band_ok = (seg_gap >= 0) & (seg_gap <= LEFT_SEGS)

    def one_block(totals, block_id):
        key_grads, value_grads, table_grad = totals
        first_row = (block_id * block_rows).astype(jnp.int32)
        queries = lax.dynamic_slice_in_dim(query_rows, first_row, block_rows, 0).astype(jnp.float32)
        queries = queries.reshape(block_rows, head_count, head_size)
        grads_out = lax.dynamic_slice_in_dim(out_grad, first_row, block_rows, 0).astype(jnp.float32)
        grads_out = grads_out.reshape(block_rows, head_count, head_size)
        log_rows = lax.dynamic_slice_in_dim(log_totals, first_row, block_rows, 0)
        dot_rows = lax.dynamic_slice_in_dim(out_dot, first_row, block_rows, 0)
        keys = lax.dynamic_slice_in_dim(padded_keys, first_row, window, 0).astype(jnp.float32)
        keys = keys.reshape(window, head_count, head_size)
        values = lax.dynamic_slice_in_dim(padded_values, first_row, window, 0).astype(jnp.float32)
        values = values.reshape(window, head_count, head_size)
        allowed = band_ok & ((first_row - lag_rows + local_key) >= 0)[None, :]
        scores = jnp.einsum('phd,rhd->hpr', queries, keys) * inv_root + bias_vals
        weights = jnp.where(allowed[None], jnp.exp(scores - log_rows.T[:, :, None]), 0.0)
        weights_b = lax.optimization_barrier(weights.astype(jnp.bfloat16)).astype(jnp.float32)
        weight_grads = jnp.einsum('phd,rhd->hpr', grads_out, values)
        score_grads = weights * (weight_grads - dot_rows.T[:, :, None])
        score_grads_b = lax.optimization_barrier(score_grads.astype(jnp.bfloat16)).astype(jnp.float32)
        block_query = jnp.einsum('hpr,rhd->phd', score_grads_b, keys) * inv_root
        block_key = (jnp.einsum('hpr,phd->rhd', score_grads_b, queries) * inv_root).reshape(window, feature_count)
        block_value = jnp.einsum('hpr,phd->rhd', weights_b, grads_out).reshape(window, feature_count)
        table_part = jax.ops.segment_sum(score_grads.reshape(head_count, -1).T, table_index.reshape(-1),
                                         num_segments=TABLE_LEN).T
        key_grads = lax.dynamic_update_slice_in_dim(
            key_grads, lax.dynamic_slice_in_dim(key_grads, first_row, window, 0) + block_key, first_row, 0)
        value_grads = lax.dynamic_update_slice_in_dim(
            value_grads, lax.dynamic_slice_in_dim(value_grads, first_row, window, 0) + block_value, first_row, 0)
        result_rows = block_query.reshape(block_rows, feature_count).astype(jnp.bfloat16)
        return (key_grads, value_grads, table_grad + table_part), result_rows

    start_totals = (jnp.zeros((lag_rows + token_count, feature_count), jnp.float32),
                    jnp.zeros((lag_rows + token_count, feature_count), jnp.float32),
                    jnp.zeros((head_count, TABLE_LEN), jnp.float32))
    block_ids = jnp.arange(token_count // block_rows, dtype=jnp.int32)
    (key_grads, value_grads, table_grad), query_grads = lax.scan(one_block, start_totals, block_ids)
    grad_query = query_grads.reshape(token_count, feature_count)
    grad_key = key_grads[lag_rows:].astype(jnp.bfloat16)
    grad_value = value_grads[lag_rows:].astype(jnp.bfloat16)
    return (grad_query, grad_key, grad_value, table_grad)
```

```python
import functools
import math

import jax
import jax.numpy as jnp
from jax import lax
from jax.experimental import pallas as pl
from jax.experimental.pallas import tpu as pltpu
from jax.sharding import PartitionSpec as P

SEG_LEN = 64
LEFT_SEGS = 8
REL_CLIP = 256
LANES = 128
SUBL = 8
MASKED = -1e30
LOG2E = math.log2(math.e)
MESH = pl.DeviceIdType.MESH


def axis_stages(size):
    stages, stride = [], 1
    while size > 1:
        order = (8, 4, 3, 2, 5, 7) if stages else (4, 3, 2, 5, 7)
        factor = next((f for f in order if size % f == 0), size)
        stages.append((stride, factor))
        stride *= factor
        size //= factor
    return stages


def iota(shape, axis):
    return lax.broadcasted_iota(jnp.int32, shape, axis)


def turn(x, amount):
    width = x.shape[1]
    return pltpu.roll(x, amount % width, 1)


def fold_diagonals(x):
    rows = x.shape[0]
    while rows > SUBL:
        half = rows // 2
        x = x[:half] + turn(x[half:], -half)
        rows = half
    return x


def fold_rows(x):
    rows = x.shape[0]
    while rows > SUBL:
        half = rows // 2
        x = x[:half] + x[half:]
        rows = half
    return x


def sublane_turn(x, direction):
    subl = iota(x.shape, 0)
    for bit in (1, 2, 4):
        x = jnp.where((subl & bit) != 0, turn(x, direction * bit), x)
    return x


def kernel(
    sizes,
    q_hbm, k_hbm, v_hbm, g_hbm, log_hbm, dot_hbm, table_hbm,
    dq_ref, dk_ref, dv_ref, dt_ref,
    q_ref, g_ref, k_ref, v_ref, log_ref, dot_ref, table_ref, load_sem,
    stat, stat_in, qg_in, part_out, part_in, dq_own, dk_acc, dv_acc,
    bias, edge, tab, neg, const, acc_pos, acc_neg, acc_const, tab_slots,
    stat_send, stat_recv, qg_send, qg_recv, part_send, part_recv, tab_send, tab_recv,
    qg_load, flood_sem, relay_send,
):
    sp_size, tp_size = sizes
    total = sp_size * tp_size
    rows, features = q_ref.shape
    heads, table_len = table_ref.shape
    head_dim = features // heads
    inv_root = head_dim ** -0.5
    table_width = tab.shape[1]
    sp, tp = lax.axis_index("sp"), lax.axis_index("tp")
    me = sp * tp_size + tp

    def device(index):
        return (index // tp_size, lax.rem(index, tp_size))

    stages = axis_stages(total)[::-1]

    group = stages[-1][1] if stages else 1
    inside = lax.rem(me + 1, group) != 0
    sends = [None, (me >= 1) & (lax.rem(me, group) != 0), me >= 2]
    relays = (me + 2 < total) & (lax.rem(me + 2, group) == 0)

    def stage_place(stage):
        stride, factor = stage
        return lax.rem(me // stride, factor)

    def stage_peer(stage, place):
        return device(me + (place - stage_place(stage)) * stage[0])

    def columns(head):
        return pl.ds(pl.multiple_of(head * head_dim, head_dim), head_dim)

    def qg_load_copy(which, head):
        return pltpu.make_async_copy(
            (q_hbm, g_hbm)[which].at[:, columns(head)], (q_ref, g_ref)[which].at[:, columns(head)],
            qg_load.at[which, head],
        )

    def start_qg_loads(head):
        qg_load_copy(0, head).start()
        qg_load_copy(1, head).start()

    loads = [
        pltpu.make_async_copy(source, target, load_sem.at[at])
        for at, (source, target) in enumerate((
            (log_hbm, log_ref), (dot_hbm, dot_ref),
            (table_hbm, table_ref), (k_hbm, k_ref), (v_hbm, v_ref),
        ))
    ]
    start_qg_loads(0)
    for load in loads[:2]:
        load.start()

    barrier = pltpu.get_barrier_semaphore()
    count = 0
    for lag in (1, 2):
        for other in (me + lag, me - lag):
            valid = (other >= 0) & (other < total)
            count = count + jnp.where(valid, 1, 0)

            @pl.when(valid)
            def _():
                pl.semaphore_signal(barrier, inc=1, device_id=device(other), device_id_type=MESH)

    pl.loop(1, heads)(start_qg_loads)
    for load in loads[2:]:
        load.start()
    pl.semaphore_wait(barrier, count)

    def stat_copy(lag):
        return pltpu.make_async_remote_copy(
            src_ref=stat, dst_ref=stat_in.at[lag - 1],
            send_sem=stat_send.at[lag - 1], recv_sem=stat_recv.at[lag - 1],
            device_id=device(me - lag), device_id_type=MESH,
        )

    def qg_copy(lag, which, head):
        return pltpu.make_async_remote_copy(
            src_ref=(q_ref, g_ref)[which].at[:, columns(head)],
            dst_ref=qg_in.at[lag - 1, which, head],
            send_sem=qg_send.at[lag - 1, which, head], recv_sem=qg_recv.at[lag - 1, which, head],
            device_id=device(me - lag), device_id_type=MESH,
        )

    def relay_copy(which, head):
        return pltpu.make_async_remote_copy(
            src_ref=qg_in.at[1, which, head], dst_ref=qg_in.at[0, which, head],
            send_sem=relay_send.at[which, head], recv_sem=qg_recv.at[0, which, head],
            device_id=device(me + 1), device_id_type=MESH,
        )

    def relay(head):
        for which in (0, 1):
            qg_copy(2, which, head).wait_recv()
            relay_copy(which, head).start()

    def part_copy(lag, head):
        return pltpu.make_async_remote_copy(
            src_ref=part_out.at[lag - 1, head], dst_ref=part_in.at[lag - 1, head],
            send_sem=part_send.at[lag - 1, head], recv_sem=part_recv.at[lag - 1, head],
            device_id=device(me + lag), device_id_type=MESH,
        )

    def send_qg(head):
        qg_load_copy(0, head).wait()
        qg_load_copy(1, head).wait()
        for lag in (1, 2):
            @pl.when(sends[lag])
            def _():
                qg_copy(lag, 0, head).start()
                qg_copy(lag, 1, head).start()

    send_qg(0)
    for load in loads[:2]:
        load.wait()
    stat[0:heads, :] = log_ref[...] * LOG2E
    stat[heads:, :] = dot_ref[...]
    for lag in (1, 2):
        @pl.when(me >= lag)
        def _():
            stat_copy(lag).start()

    pl.loop(1, heads)(send_qg)

    reaches, reach = [], 2
    while reach < max([stride * (factor - 1) for stride, factor in stages] + [0]):
        reaches.append(reach)
        reach *= 2

    def flood_others(at):
        others = (me + reaches[at], me - reaches[at])
        return [(other, (other >= 0) & (other < total)) for other in others]

    def flood_start(at):
        if at < len(reaches):
            for other, valid in flood_others(at):
                @pl.when(valid)
                def _():
                    pl.semaphore_signal(
                        flood_sem.at[at], inc=1, device_id=device(other), device_id_type=MESH
                    )

    def flood_finish(at):
        if at < len(reaches):
            pl.semaphore_wait(
                flood_sem.at[at], sum(jnp.where(valid, 1, 0) for _, valid in flood_others(at))
            )

    flood_start(0)

    loads[2].wait()
    tab[...] = jnp.zeros_like(tab)
    tab[:, 0:table_len] = table_ref[...] * LOG2E
    padded = tab[...]
    from_zero = turn(padded, 1 - SEG_LEN)
    neg[...] = turn(padded, LANES - (SEG_LEN - 1))[:, 0:LANES]
    const[...] = jnp.broadcast_to(from_zero[:, rows:rows + 1], const.shape)
    tab[...] = from_zero
    key_at, query_at = iota((rows, rows), 0), iota((rows, rows), 1)
    edge[...] = jnp.where(query_at // SEG_LEN <= key_at // SEG_LEN, 0.0, MASKED)

    @pl.loop(0, heads)
    def _(head):
        row = jnp.broadcast_to(tab[pl.ds(head, 1), 0:rows], (SUBL, rows))
        near = sublane_turn(row, 1)
        row = jnp.broadcast_to(neg[pl.ds(head, 1), :], (SUBL, LANES))
        before = sublane_turn(row, 1)
        have = SUBL
        while have < rows:
            near = jnp.concatenate([near, turn(near, have)], axis=0)
            if have < LANES:
                before = jnp.concatenate([before, turn(before, have)], axis=0)
            have *= 2
        far = const[pl.ds(head, 1), :]
        upper = iota((rows, rows), 1) >= iota((rows, rows), 0)
        bias[1, head] = jnp.where(upper, far, near)
        segs_ok = iota((rows, rows), 1) // SEG_LEN >= iota((rows, rows), 0) // SEG_LEN
        wide = jnp.concatenate([before] * (rows // LANES), axis=1)
        tall = jnp.concatenate([wide] * (rows // LANES), axis=0)
        bias[0, head] = jnp.where(upper, near, jnp.where(segs_ok, tall, MASKED))

    def pair_terms(lag, head, queries, grads, log_row, dot_row):
        keys, values = k_ref[:, columns(head)], v_ref[:, columns(head)]
        across = (((1,), (1,)), ((), ()))
        scores = lax.dot_general(keys, queries, across, preferred_element_type=jnp.float32)
        if lag < 2:
            shift = bias[lag, head] - log_row
        else:
            shift = edge[...] + (const[pl.ds(head, 1), :] - log_row)
        weights = jnp.exp2(scores * (inv_root * LOG2E) + shift)
        weight_grads = lax.dot_general(values, grads, across, preferred_element_type=jnp.float32)
        score_grads = weights * (weight_grads - dot_row)
        score_grads_b = score_grads.astype(jnp.bfloat16)
        value_part = jnp.dot(
            weights.astype(jnp.bfloat16), grads, preferred_element_type=jnp.float32
        )
        key_part = jnp.dot(score_grads_b, queries, preferred_element_type=jnp.float32)
        query_part = lax.dot_general(
            score_grads_b, keys, (((0,), (0,)), ((), ())), preferred_element_type=jnp.float32
        )
        return score_grads, query_part, key_part, value_part

    loads[3].wait()
    loads[4].wait()
    in_loop = min(len(reaches), heads // 2)

    @pl.loop(0, heads)
    def _(head):
        score_grads, query_part, key_part, value_part = pair_terms(
            0, head, q_ref[:, columns(head)], g_ref[:, columns(head)],
            stat[pl.ds(head, 1), :], stat[pl.ds(head + heads, 1), :],
        )
        dq_own[head] = query_part
        dk_acc[head] = key_part
        dv_acc[head] = value_part
        upper = iota((rows, rows), 1) >= iota((rows, rows), 0)
        acc_pos[head] = fold_diagonals(jnp.where(upper, score_grads, 0.0))
        lower = jnp.where(upper, 0.0, score_grads)
        tiles = sum(
            lower[at:at + LANES, at:at + LANES] for at in range(0, rows, LANES)
        )
        acc_neg[head] = fold_diagonals(tiles)
        acc_const[head] = jnp.zeros(acc_const.shape[1:], jnp.float32)
        @pl.when(relays & (lax.rem(head, 2) == 1))
        def _():
            relay(head // 2)

        for at in range(in_loop):
            @pl.when(head == 2 * at + 1)
            def _():
                flood_finish(at)
                flood_start(at + 1)

    def start_parts(first, last):
        @pl.loop(first, last)
        def _(head):
            part_copy(1, head).start()

    for at in range(in_loop, len(reaches)):
        flood_finish(at)
        flood_start(at + 1)

    for lag in (2, 1):
        @pl.when(me + lag < total)
        def _():
            stat_copy(lag).wait_recv()

    @pl.loop(0, heads)
    def _(head):
        @pl.when(relays & (head < heads - heads // 2))
        def _():
            relay(head + heads // 2)

        for lag in (2, 1):
            @pl.when(me + lag < total)
            def _():
                @pl.when((lag == 1) | ~relays)
                def _():
                    qg_copy(lag, 0, head).wait_recv()
                    qg_copy(lag, 1, head).wait_recv()

                score_grads, query_part, key_part, value_part = pair_terms(
                    lag, head, qg_in[lag - 1, 0, head], qg_in[lag - 1, 1, head],
                    stat_in[lag - 1, pl.ds(head, 1), :],
                    stat_in[lag - 1, pl.ds(head + heads, 1), :],
                )
                part_out[lag - 1, head] = query_part.astype(jnp.bfloat16)
                if lag == 2:
                    part_copy(2, head).start()
                dk_acc[head] += key_part
                dv_acc[head] += value_part
                if lag == 1:
                    upper = iota((rows, rows), 1) >= iota((rows, rows), 0)
                    acc_const[head] += fold_rows(jnp.where(upper, score_grads, 0.0))
                    acc_pos[head] += fold_diagonals(jnp.where(upper, 0.0, score_grads))
                else:
                    acc_const[head] += fold_rows(score_grads)

        @pl.when((me + 1 < total) & inside & (head == heads - 2))
        def _():
            start_parts(0, heads - 1)

        dk_ref[:, columns(head)] = (dk_acc[head] * inv_root).astype(dk_ref.dtype)
        dv_ref[:, columns(head)] = dv_acc[head].astype(dv_ref.dtype)
        near = jnp.sum(sublane_turn(acc_pos[head], -1), axis=0, keepdims=True)
        before = jnp.sum(sublane_turn(acc_neg[head], -1), axis=0, keepdims=True)
        far = jnp.sum(jnp.sum(acc_const[head], axis=0, keepdims=True), axis=1, keepdims=True)
        tail = jnp.broadcast_to(far, (1, table_width - rows))
        tail = jnp.where(iota(tail.shape, 1) == 0, tail, 0.0)
        here = iota(tab.shape, 0) == head
        tab[...] = jnp.where(here, jnp.concatenate([near, tail], axis=1), tab[...])
        neg[...] = jnp.where(iota(neg.shape, 0) == head, before, neg[...])

    spread = jnp.concatenate(
        [neg[...], jnp.zeros((heads, table_width - LANES), jnp.float32)], axis=1
    )
    running = turn(tab[...], SEG_LEN - 1) + turn(spread, -(LANES - (SEG_LEN - 1)))

    def tab_copy(at, place, peer_place):
        stage = stages[at]
        return pltpu.make_async_remote_copy(
            src_ref=tab_slots.at[at, place], dst_ref=tab_slots.at[at, place],
            send_sem=tab_send.at[at, peer_place], recv_sem=tab_recv.at[at, place],
            device_id=stage_peer(stage, peer_place), device_id_type=MESH,
        )

    def stage_start(at, block):
        place = stage_place(stages[at])
        tab_slots[at, place] = block
        for offset in range(1, stages[at][1]):
            tab_copy(at, place, lax.rem(place + offset, stages[at][1])).start()

    def stage_finish(at):
        factor = stages[at][1]
        place = stage_place(stages[at])
        for offset in range(1, factor):
            other = lax.rem(place + offset, factor)
            tab_copy(at, other, other).wait_recv()
        out = tab_slots[at, 0]
        for member in range(1, factor):
            out = out + tab_slots[at, member]
        return out

    def finish_queries(first, last):
        @pl.loop(first, last)
        def _(head):
            for lag in (2, 1):
                @pl.when(me >= lag)
                def _():
                    part_copy(lag, head).wait_recv()
                    dq_own[head] += part_in[lag - 1, head].astype(jnp.float32)
            dq_ref[:, columns(head)] = (dq_own[head] * inv_root).astype(dq_ref.dtype)

    if stages:
        stage_start(0, running)

    @pl.when((me + 1 < total) & ~inside)
    def _():
        start_parts(0, heads)

    for at in range(len(stages) - 1):
        stage_start(at + 1, stage_finish(at))

    @pl.when((me + 1 < total) & inside)
    def _():
        start_parts(heads - 1, heads)

    finish_queries(0, heads)
    if stages:
        running = stage_finish(len(stages) - 1)
    dt_ref[...] = running[:, 0:table_len]

    for lag in (1, 2):
        @pl.when(me >= lag)
        def _():
            stat_copy(lag).wait_send()

    @pl.loop(0, heads)
    def _(head):
        for lag in (1, 2):
            @pl.when(sends[lag])
            def _():
                qg_copy(lag, 0, head).wait_send()
                qg_copy(lag, 1, head).wait_send()

            @pl.when(me + lag < total)
            def _():
                part_copy(lag, head).wait_send()

        @pl.when(relays)
        def _():
            relay_copy(0, head).wait_send()
            relay_copy(1, head).wait_send()

    for at, stage in enumerate(stages):
        place = stage_place(stage)
        for offset in range(1, stage[1]):
            tab_copy(at, place, lax.rem(place + offset, stage[1])).wait_send()


def store_kernel(*refs):
    sources, targets, sem = refs[:4], refs[4:8], refs[8]
    stores = [pltpu.make_async_copy(sources[at], targets[at], sem.at[at]) for at in range(4)]
    for store in stores:
        store.start()
    for store in stores:
        store.wait()


def local(sizes, query_rows, key_rows, value_rows, out_grad, log_totals, out_dot, bias_table):
    rows, features = query_rows.shape
    heads, table_len = bias_table.shape
    head_dim = features // heads
    assert LEFT_SEGS * SEG_LEN == 2 * rows and rows == REL_CLIP
    assert table_len == REL_CLIP + SEG_LEN and head_dim == LANES
    stage_list = axis_stages(sizes[0] * sizes[1])
    stage_count = max(len(stage_list), 1)
    slot_count = max([factor for _, factor in stage_list] + [1])
    table_width = -(-(table_len + 1) // LANES) * LANES
    f32, bf16 = jnp.float32, jnp.bfloat16
    vmem = pl.BlockSpec(memory_space=pltpu.VMEM)
    dma = pltpu.SemaphoreType.DMA
    wide = pltpu.VMEM((rows, features), bf16)
    results = pl.pallas_call(
        functools.partial(kernel, sizes),
        out_shape=(wide, wide, wide, pltpu.VMEM((heads, table_len), f32)),
        in_specs=[pl.BlockSpec(memory_space=pltpu.HBM)] * 7,
        out_specs=(vmem,) * 4,
        scratch_shapes=[
            pltpu.VMEM((rows, features), bf16),
            pltpu.VMEM((rows, features), bf16),
            pltpu.VMEM((rows, features), bf16),
            pltpu.VMEM((rows, features), bf16),
            pltpu.VMEM((heads, rows), f32),
            pltpu.VMEM((heads, rows), f32),
            pltpu.VMEM((heads, table_len), f32),
            dma((5,)),
            pltpu.VMEM((2 * heads, rows), f32),
            pltpu.VMEM((2, 2 * heads, rows), f32),
            pltpu.VMEM((2, 2, heads, rows, head_dim), bf16),
            pltpu.VMEM((2, heads, rows, head_dim), bf16),
            pltpu.VMEM((2, heads, rows, head_dim), bf16),
            pltpu.VMEM((heads, rows, head_dim), f32),
            pltpu.VMEM((heads, rows, head_dim), f32),
            pltpu.VMEM((heads, rows, head_dim), f32),
            pltpu.VMEM((2, heads, rows, rows), f32),
            pltpu.VMEM((rows, rows), f32),
            pltpu.VMEM((heads, table_width), f32),
            pltpu.VMEM((heads, LANES), f32),
            pltpu.VMEM((heads, rows), f32),
            pltpu.VMEM((heads, SUBL, rows), f32),
            pltpu.VMEM((heads, SUBL, LANES), f32),
            pltpu.VMEM((heads, SUBL, rows), f32),
            pltpu.VMEM((stage_count, slot_count, heads, table_width), f32),
            dma((2,)), dma((2,)),
            dma((2, 2, heads)), dma((2, 2, heads)),
            dma((2, heads)), dma((2, heads)),
            dma((stage_count, slot_count)), dma((stage_count, slot_count)),
            dma((2, heads)), pltpu.SemaphoreType.REGULAR((16,)), dma((2, heads)),
        ],
        compiler_params=pltpu.CompilerParams(
            collective_id=0, has_side_effects=True, vmem_limit_bytes=40 * 2**20
        ),
        name="band_backward",
    )(*(pltpu.with_memory_space_constraint(x, pltpu.HBM) for x in (query_rows, key_rows, value_rows, out_grad, log_totals.T, out_dot.T, bias_table)))
    return pl.pallas_call(
        store_kernel,
        out_shape=tuple(jax.ShapeDtypeStruct(x.shape, x.dtype) for x in results),
        in_specs=[vmem] * 4,
        out_specs=(pl.BlockSpec(memory_space=pltpu.HBM),) * 4,
        scratch_shapes=[dma((4,))],
        compiler_params=pltpu.CompilerParams(vmem_limit_bytes=2**20),
        name="store",
    )(*results)


def solution(mesh):
    sizes = (mesh.shape["sp"], mesh.shape["tp"])
    by_rows = P(("sp", "tp"), None)
    return jax.shard_map(
        functools.partial(local, sizes),
        mesh=mesh,
        in_specs=(by_rows,) * 6 + (P(),),
        out_specs=(by_rows, by_rows, by_rows, P()),
        check_vma=False,
    )
```

```python
import functools
import math

import jax
import jax.numpy as jnp
from jax import lax
from jax.experimental import pallas as pl
from jax.experimental.pallas import tpu as pltpu
from jax.sharding import PartitionSpec as P

SEG_LEN = 64
LEFT_SEGS = 8
REL_CLIP = 256
LANES = 128
SUBL = 8
MASKED = -1e30
LOG2E = math.log2(math.e)
MESH = pl.DeviceIdType.MESH


def axis_stages(size):
    stages, stride = [], 1
    while size > 1:
        order = (8, 4, 3, 2, 5, 7) if stages else (4, 3, 2, 5, 7)
        factor = next((f for f in order if size % f == 0), size)
        stages.append((stride, factor))
        stride *= factor
        size //= factor
    return stages


def flood_reaches(stages):
    reaches, reach = [], 2
    while reach < max([stride * (factor - 1) for stride, factor in stages] + [0]):
        reaches.append(reach)
        reach *= 2
    return reaches


def iota(shape, axis):
    return lax.broadcasted_iota(jnp.int32, shape, axis)


def turn(x, amount):
    width = x.shape[1]
    return pltpu.roll(x, amount % width, 1)


def fold_diagonals(x):
    rows = x.shape[0]
    while rows > SUBL:
        half = rows // 2
        x = x[:half] + turn(x[half:], -half)
        rows = half
    return x


def fold_rows(x):
    rows = x.shape[0]
    while rows > SUBL:
        half = rows // 2
        x = x[:half] + x[half:]
        rows = half
    return x


def sublane_turn(x, direction):
    subl = iota(x.shape, 0)
    for bit in (1, 2, 4):
        x = jnp.where((subl & bit) != 0, turn(x, direction * bit), x)
    return x


def kernel(
    sizes,
    q_hbm, k_hbm, v_hbm, g_hbm, log_hbm, dot_hbm, table_hbm,
    dq_ref, dk_ref, dv_ref, dt_ref,
    qg_ref, kv_ref, rows_ref, table_ref, load_sem,
    stat, stat_in, qg_in, part_out, part_in, dq_own, dk_acc, dv_acc,
    bias, edge, tab, neg, const, acc_pos, acc_neg, acc_const, tab_slots,
    stat_send, stat_recv, qg_send, qg_recv, part_send, part_recv, tab_send, tab_recv,
    flood_sem, relay_send,
):
    sp_size, tp_size = sizes
    total = sp_size * tp_size
    _, rows, features = qg_ref.shape
    heads, table_len = table_ref.shape
    head_dim = features // heads
    inv_root = head_dim ** -0.5
    table_width = tab.shape[1]
    sp, tp = lax.axis_index("sp"), lax.axis_index("tp")
    me = sp * tp_size + tp

    def device(index):
        return (index // tp_size, lax.rem(index, tp_size))

    stages = axis_stages(total)[::-1]

    group = stages[-1][1] if stages else 1
    inside = lax.rem(me + 1, group) != 0
    held = min(2, heads)
    sends = [None, (me >= 1) & (lax.rem(me, group) != 0), me >= 2]
    relays = (me + 2 < total) & (lax.rem(me + 2, group) == 0)

    def stage_place(stage):
        stride, factor = stage
        return lax.rem(me // stride, factor)

    def stage_peer(stage, place):
        return device(me + (place - stage_place(stage)) * stage[0])

    def columns(head):
        return pl.ds(pl.multiple_of(head * head_dim, head_dim), head_dim)

    first, others = pl.ds(0, head_dim), pl.ds(head_dim, features - head_dim)
    stat_rows = (pl.ds(0, heads), pl.ds(heads, heads))
    loads = [
        [(q_hbm.at[:, first], qg_ref.at[0, :, first]), (g_hbm.at[:, first], qg_ref.at[1, :, first])],
        [(log_hbm, rows_ref.at[stat_rows[0]]), (dot_hbm, rows_ref.at[stat_rows[1]])],
        [(q_hbm.at[:, others], qg_ref.at[0, :, others]), (g_hbm.at[:, others], qg_ref.at[1, :, others])],
        [(table_hbm, table_ref)],
        [(k_hbm, kv_ref.at[0]), (v_hbm, kv_ref.at[1])],
    ]
    loaded = [qg_ref.at[:, :, first], rows_ref, qg_ref.at[:, :, others], table_ref, kv_ref]

    def load_start(at):
        for source, target in loads[at]:
            pltpu.make_async_copy(source, target, load_sem.at[at]).start()

    def load_wait(at):
        pltpu.make_async_copy(loaded[at], loaded[at], load_sem.at[at]).wait()

    load_start(0)
    load_start(1)

    barrier = pltpu.get_barrier_semaphore()
    count = 0
    for lag in (1, 2):
        for other in (me + lag, me - lag):
            valid = (other >= 0) & (other < total)
            count = count + jnp.where(valid, 1, 0)

            @pl.when(valid)
            def _():
                pl.semaphore_signal(barrier, inc=1, device_id=device(other), device_id_type=MESH)

    for at in range(2, len(loads)):
        load_start(at)
    pl.semaphore_wait(barrier, count)

    def stat_copy(lag):
        return pltpu.make_async_remote_copy(
            src_ref=stat, dst_ref=stat_in.at[lag - 1],
            send_sem=stat_send.at[lag - 1], recv_sem=stat_recv.at[lag - 1],
            device_id=device(me - lag), device_id_type=MESH,
        )

    def qg_copy(lag, head):
        return pltpu.make_async_remote_copy(
            src_ref=qg_ref.at[:, :, columns(head)], dst_ref=qg_in.at[lag - 1, head],
            send_sem=qg_send.at[lag - 1], recv_sem=qg_recv.at[lag - 1, head],
            device_id=device(me - lag), device_id_type=MESH,
        )

    def relay_copy(head):
        return pltpu.make_async_remote_copy(
            src_ref=qg_in.at[1, head], dst_ref=qg_in.at[0, head],
            send_sem=relay_send.at[0], recv_sem=qg_recv.at[0, head],
            device_id=device(me + 1), device_id_type=MESH,
        )

    def relay(head):
        qg_copy(2, head).wait_recv()
        relay_copy(head).start()

    def part_copy(lag, head):
        return pltpu.make_async_remote_copy(
            src_ref=part_out.at[lag - 1, head], dst_ref=part_in.at[lag - 1, head],
            send_sem=part_send.at[lag - 1],
            recv_sem=part_recv.at[head if lag == 1 else heads],
            device_id=device(me + lag), device_id_type=MESH,
        )

    def whole(ref, send_sem, recv_sem):
        return pltpu.make_async_remote_copy(
            src_ref=ref, dst_ref=ref, send_sem=send_sem, recv_sem=recv_sem,
            device_id=device(me), device_id_type=MESH,
        )

    def send_qg(head):
        for lag in (1, 2):
            @pl.when(sends[lag])
            def _():
                qg_copy(lag, head).start()

    load_wait(0)
    send_qg(0)
    load_wait(1)
    stat[0:heads, :] = rows_ref[0:heads, :] * LOG2E
    stat[heads:, :] = rows_ref[heads:, :]
    for lag in (1, 2):
        @pl.when(me >= lag)
        def _():
            stat_copy(lag).start()

    load_wait(2)
    pl.loop(1, heads)(send_qg)

    reaches = flood_reaches(stages)

    def flood_others(at):
        others = (me + reaches[at], me - reaches[at])
        return [(other, (other >= 0) & (other < total)) for other in others]

    def flood_start(at):
        if at < len(reaches):
            for other, valid in flood_others(at):
                @pl.when(valid)
                def _():
                    pl.semaphore_signal(
                        flood_sem.at[at], inc=1, device_id=device(other), device_id_type=MESH
                    )

    def flood_finish(at):
        if at < len(reaches):
            pl.semaphore_wait(
                flood_sem.at[at], sum(jnp.where(valid, 1, 0) for _, valid in flood_others(at))
            )

    flood_start(0)

    load_wait(3)
    tab[...] = jnp.zeros_like(tab)
    tab[:, 0:table_len] = table_ref[...] * LOG2E
    padded = tab[...]
    from_zero = turn(padded, 1 - SEG_LEN)
    neg[...] = turn(padded, LANES - (SEG_LEN - 1))[:, 0:LANES]
    const[...] = jnp.broadcast_to(from_zero[:, rows:rows + 1], const.shape)
    tab[...] = from_zero
    key_at, query_at = iota((rows, rows), 0), iota((rows, rows), 1)
    edge[...] = jnp.where(query_at // SEG_LEN <= key_at // SEG_LEN, 0.0, MASKED)

    @pl.loop(0, heads)
    def _(head):
        row = jnp.broadcast_to(tab[pl.ds(head, 1), 0:rows], (SUBL, rows))
        near = sublane_turn(row, 1)
        row = jnp.broadcast_to(neg[pl.ds(head, 1), :], (SUBL, LANES))
        before = sublane_turn(row, 1)
        have = SUBL
        while have < rows:
            near = jnp.concatenate([near, turn(near, have)], axis=0)
            if have < LANES:
                before = jnp.concatenate([before, turn(before, have)], axis=0)
            have *= 2
        far = const[pl.ds(head, 1), :]
        upper = iota((rows, rows), 1) >= iota((rows, rows), 0)
        bias[1, head] = jnp.where(upper, far, near)
        segs_ok = iota((rows, rows), 1) // SEG_LEN >= iota((rows, rows), 0) // SEG_LEN
        wide = jnp.concatenate([before] * (rows // LANES), axis=1)
        tall = jnp.concatenate([wide] * (rows // LANES), axis=0)
        bias[0, head] = jnp.where(upper, near, jnp.where(segs_ok, tall, MASKED))

    def pair_terms(lag, head, queries, grads, log_row, dot_row):
        keys, values = kv_ref[0, :, columns(head)], kv_ref[1, :, columns(head)]
        across = (((1,), (1,)), ((), ()))
        scores = lax.dot_general(keys, queries, across, preferred_element_type=jnp.float32)
        if lag < 2:
            shift = bias[lag, head] - log_row
        else:
            shift = edge[...] + (const[pl.ds(head, 1), :] - log_row)
        weights = jnp.exp2(scores * (inv_root * LOG2E) + shift)
        weight_grads = lax.dot_general(values, grads, across, preferred_element_type=jnp.float32)
        score_grads = weights * (weight_grads - dot_row)
        score_grads_b = score_grads.astype(jnp.bfloat16)
        value_part = jnp.dot(
            weights.astype(jnp.bfloat16), grads, preferred_element_type=jnp.float32
        )
        key_part = jnp.dot(score_grads_b, queries, preferred_element_type=jnp.float32)
        query_part = lax.dot_general(
            score_grads_b, keys, (((0,), (0,)), ((), ())), preferred_element_type=jnp.float32
        )
        return score_grads, query_part, key_part, value_part

    load_wait(4)
    in_loop = min(len(reaches), heads // 2)

    @pl.loop(0, heads)
    def _(head):
        score_grads, query_part, key_part, value_part = pair_terms(
            0, head, qg_ref[0, :, columns(head)], qg_ref[1, :, columns(head)],
            stat[pl.ds(head, 1), :], stat[pl.ds(head + heads, 1), :],
        )
        dq_own[head] = query_part
        dk_acc[head] = key_part
        dv_acc[head] = value_part
        upper = iota((rows, rows), 1) >= iota((rows, rows), 0)
        acc_pos[head] = fold_diagonals(jnp.where(upper, score_grads, 0.0))
        lower = jnp.where(upper, 0.0, score_grads)
        tiles = sum(
            lower[at:at + LANES, at:at + LANES] for at in range(0, rows, LANES)
        )
        acc_neg[head] = fold_diagonals(tiles)
        acc_const[head] = jnp.zeros(acc_const.shape[1:], jnp.float32)

        @pl.when(relays & (lax.rem(head, 2) == 1))
        def _():
            relay(head // 2)

        for at in range(in_loop):
            @pl.when(head == 2 * at + 1)
            def _():
                flood_finish(at)
                flood_start(at + 1)

    def start_parts(first, last):
        @pl.loop(first, last)
        def _(head):
            part_copy(1, head).start()

    for at in range(in_loop, len(reaches)):
        flood_finish(at)
        flood_start(at + 1)

    for lag in (2, 1):
        @pl.when(me + lag < total)
        def _():
            stat_copy(lag).wait_recv()

    @pl.loop(0, heads)
    def _(head):
        @pl.when(relays & (head < heads - heads // 2))
        def _():
            relay(head + heads // 2)

        for lag in (2, 1):
            @pl.when(me + lag < total)
            def _():
                @pl.when((lag == 1) | ~relays)
                def _():
                    qg_copy(lag, head).wait_recv()

                score_grads, query_part, key_part, value_part = pair_terms(
                    lag, head, qg_in[lag - 1, head, 0], qg_in[lag - 1, head, 1],
                    stat_in[lag - 1, pl.ds(head, 1), :],
                    stat_in[lag - 1, pl.ds(head + heads, 1), :],
                )
                part_out[lag - 1, head] = query_part.astype(jnp.bfloat16)
                if lag == 2:
                    part_copy(2, head).start()
                dk_acc[head] += key_part
                dv_acc[head] += value_part
                if lag == 1:
                    upper = iota((rows, rows), 1) >= iota((rows, rows), 0)
                    acc_const[head] += fold_rows(jnp.where(upper, score_grads, 0.0))
                    acc_pos[head] += fold_diagonals(jnp.where(upper, 0.0, score_grads))
                else:
                    acc_const[head] += fold_rows(score_grads)

        @pl.when((me + 1 < total) & inside & (head == heads - 2))
        def _():
            start_parts(0, heads - held)

        dk_ref[:, columns(head)] = (dk_acc[head] * inv_root).astype(dk_ref.dtype)
        dv_ref[:, columns(head)] = dv_acc[head].astype(dv_ref.dtype)
        near = jnp.sum(sublane_turn(acc_pos[head], -1), axis=0, keepdims=True)
        before = jnp.sum(sublane_turn(acc_neg[head], -1), axis=0, keepdims=True)
        far = jnp.sum(jnp.sum(acc_const[head], axis=0, keepdims=True), axis=1, keepdims=True)
        tail = jnp.broadcast_to(far, (1, table_width - rows))
        tail = jnp.where(iota(tail.shape, 1) == 0, tail, 0.0)
        here = iota(tab.shape, 0) == head
        tab[...] = jnp.where(here, jnp.concatenate([near, tail], axis=1), tab[...])
        neg[...] = jnp.where(iota(neg.shape, 0) == head, before, neg[...])

    spread = jnp.concatenate(
        [neg[...], jnp.zeros((heads, table_width - LANES), jnp.float32)], axis=1
    )
    running = turn(tab[...], SEG_LEN - 1) + turn(spread, -(LANES - (SEG_LEN - 1)))

    def tab_copy(at, place, peer_place):
        stage = stages[at]
        return pltpu.make_async_remote_copy(
            src_ref=tab_slots.at[at, place], dst_ref=tab_slots.at[at, place],
            send_sem=tab_send.at[at], recv_sem=tab_recv.at[at],
            device_id=stage_peer(stage, peer_place), device_id_type=MESH,
        )

    def stage_start(at, block):
        place = stage_place(stages[at])
        tab_slots[at, place] = block
        for offset in range(1, stages[at][1]):
            tab_copy(at, place, lax.rem(place + offset, stages[at][1])).start()

    def stage_finish(at):
        factor = stages[at][1]
        peers = tab_slots.at[at, pl.ds(0, factor - 1)]
        whole(peers, tab_send.at[at], tab_recv.at[at]).wait_recv()
        out = tab_slots[at, 0]
        for member in range(1, factor):
            out = out + tab_slots[at, member]
        return out

    if stages:
        stage_start(0, running)

    @pl.when((me + 1 < total) & ~inside)
    def _():
        start_parts(0, heads - held)

    for at in range(len(stages) - 1):
        stage_start(at + 1, stage_finish(at))

    @pl.when(me + 1 < total)
    def _():
        start_parts(heads - held, heads)

    @pl.when(me >= 2)
    def _():
        whole(part_in.at[1], part_send.at[1], part_recv.at[heads]).wait_recv()

        @pl.loop(0, heads)
        def _(head):
            dq_own[head] += part_in[1, head].astype(jnp.float32)

    @pl.loop(0, heads)
    def _(head):
        @pl.when(me >= 1)
        def _():
            part_copy(1, head).wait_recv()
            dq_own[head] += part_in[0, head].astype(jnp.float32)

        dq_ref[:, columns(head)] = (dq_own[head] * inv_root).astype(dq_ref.dtype)

    if stages:
        running = stage_finish(len(stages) - 1)
    dt_ref[...] = running[:, 0:table_len]

    for lag in (1, 2):
        @pl.when(me >= lag)
        def _():
            stat_copy(lag).wait_send()

        @pl.when(sends[lag])
        def _():
            whole(qg_ref, qg_send.at[lag - 1], qg_recv.at[lag - 1, 0]).wait_send()

        @pl.when(me + lag < total)
        def _():
            whole(part_out.at[lag - 1], part_send.at[lag - 1], part_recv.at[0]).wait_send()

    @pl.when(relays)
    def _():
        whole(qg_in.at[1], relay_send.at[0], qg_recv.at[0, 0]).wait_send()

    for at, (_, factor) in enumerate(stages):
        peers = tab_slots.at[at, pl.ds(0, factor - 1)]
        whole(peers, tab_send.at[at], tab_recv.at[at]).wait_send()


def store_kernel(*refs):
    sources, targets, sem = refs[:4], refs[4:8], refs[8]
    stores = [pltpu.make_async_copy(sources[at], targets[at], sem.at[at]) for at in range(4)]
    for store in stores:
        store.start()
    for store in stores:
        store.wait()


def local(sizes, query_rows, key_rows, value_rows, out_grad, log_totals, out_dot, bias_table):
    rows, features = query_rows.shape
    heads, table_len = bias_table.shape
    head_dim = features // heads
    assert LEFT_SEGS * SEG_LEN == 2 * rows and rows == REL_CLIP
    assert table_len == REL_CLIP + SEG_LEN and head_dim == LANES
    stage_list = axis_stages(sizes[0] * sizes[1])
    stage_count = max(len(stage_list), 1)
    flood_count = max(len(flood_reaches(stage_list)), 1)
    slot_count = max([factor for _, factor in stage_list] + [1])
    table_width = -(-(table_len + 1) // LANES) * LANES
    f32, bf16 = jnp.float32, jnp.bfloat16
    vmem = pl.BlockSpec(memory_space=pltpu.VMEM)
    dma = pltpu.SemaphoreType.DMA
    wide = pltpu.VMEM((rows, features), bf16)
    results = pl.pallas_call(
        functools.partial(kernel, sizes),
        out_shape=(wide, wide, wide, pltpu.VMEM((heads, table_len), f32)),
        in_specs=[pl.BlockSpec(memory_space=pltpu.HBM)] * 7,
        out_specs=(vmem,) * 4,
        scratch_shapes=[
            pltpu.VMEM((2, rows, features), bf16),
            pltpu.VMEM((2, rows, features), bf16),
            pltpu.VMEM((2 * heads, rows), f32),
            pltpu.VMEM((heads, table_len), f32),
            dma((5,)),
            pltpu.VMEM((2 * heads, rows), f32),
            pltpu.VMEM((2, 2 * heads, rows), f32),
            pltpu.VMEM((2, heads, 2, rows, head_dim), bf16),
            pltpu.VMEM((2, heads, rows, head_dim), bf16),
            pltpu.VMEM((2, heads, rows, head_dim), bf16),
            pltpu.VMEM((heads, rows, head_dim), f32),
            pltpu.VMEM((heads, rows, head_dim), f32),
            pltpu.VMEM((heads, rows, head_dim), f32),
            pltpu.VMEM((2, heads, rows, rows), f32),
            pltpu.VMEM((rows, rows), f32),
            pltpu.VMEM((heads, table_width), f32),
            pltpu.VMEM((heads, LANES), f32),
            pltpu.VMEM((heads, rows), f32),
            pltpu.VMEM((heads, SUBL, rows), f32),
            pltpu.VMEM((heads, SUBL, LANES), f32),
            pltpu.VMEM((heads, SUBL, rows), f32),
            pltpu.VMEM((stage_count, slot_count, heads, table_width), f32),
            dma((2,)), dma((2,)),
            dma((2,)), dma((2, heads)),
            dma((2,)), dma((heads + 1,)),
            dma((stage_count,)), dma((stage_count,)),
            pltpu.SemaphoreType.REGULAR((flood_count,)), dma((1,)),
        ],
        compiler_params=pltpu.CompilerParams(
            collective_id=0, has_side_effects=True, vmem_limit_bytes=40 * 2**20
        ),
        name="band_backward",
    )(*(pltpu.with_memory_space_constraint(x, pltpu.HBM) for x in (query_rows, key_rows, value_rows, out_grad, log_totals.T, out_dot.T, bias_table)))
    return pl.pallas_call(
        store_kernel,
        out_shape=tuple(jax.ShapeDtypeStruct(x.shape, x.dtype) for x in results),
        in_specs=[vmem] * 4,
        out_specs=(pl.BlockSpec(memory_space=pltpu.HBM),) * 4,
        scratch_shapes=[dma((4,))],
        compiler_params=pltpu.CompilerParams(vmem_limit_bytes=2**20),
        name="store",
    )(*results)


def solution(mesh):
    sizes = (mesh.shape["sp"], mesh.shape["tp"])
    by_rows = P(("sp", "tp"), None)
    return jax.shard_map(
        functools.partial(local, sizes),
        mesh=mesh,
        in_specs=(by_rows,) * 6 + (P(),),
        out_specs=(by_rows, by_rows, by_rows, P()),
        check_vma=False,
    )
```

```python
import functools
import math

import jax
import jax.numpy as jnp
from jax import lax
from jax.experimental import pallas as pl
from jax.experimental.pallas import tpu as pltpu
from jax.sharding import PartitionSpec as P

SEG_LEN = 64
LEFT_SEGS = 8
REL_CLIP = 256
LANES = 128
SUBL = 8
MASKED = -1e30
LOG2E = math.log2(math.e)
MESH = pl.DeviceIdType.MESH


def axis_stages(size):
    stages, stride = [], 1
    while size > 1:
        order = (8, 4, 3, 2, 5, 7) if stages else (4, 3, 2, 5, 7)
        factor = next((f for f in order if size % f == 0), size)
        stages.append((stride, factor))
        stride *= factor
        size //= factor
    return stages


def flood_reaches(stages):
    reaches, reach = [], 2
    while reach < max([stride * (factor - 1) for stride, factor in stages] + [0]):
        reaches.append(reach)
        reach *= 2
    return reaches


def iota(shape, axis):
    return lax.broadcasted_iota(jnp.int32, shape, axis)


def turn(x, amount):
    width = x.shape[1]
    return pltpu.roll(x, amount % width, 1)


def fold_diagonals(x):
    rows = x.shape[0]
    while rows > SUBL:
        half = rows // 2
        x = x[:half] + turn(x[half:], -half)
        rows = half
    return x


def fold_rows(x):
    rows = x.shape[0]
    while rows > SUBL:
        half = rows // 2
        x = x[:half] + x[half:]
        rows = half
    return x


def sublane_turn(x, direction):
    subl = iota(x.shape, 0)
    for bit in (1, 2, 4):
        x = jnp.where((subl & bit) != 0, turn(x, direction * bit), x)
    return x


def kernel(
    sizes,
    q_hbm, k_hbm, v_hbm, g_hbm, log_hbm, dot_hbm, table_hbm,
    dq_ref, dk_ref, dv_ref, dt_ref,
    qg_ref, kv_ref, rows_ref, table_ref, load_sem,
    stat, stat_in, qg_in, part_out, part_in, dq_own, dk_acc, dv_acc,
    bias, edge, tab, neg, const, acc_pos, acc_neg, acc_const, tab_slots,
    stat_send, stat_recv, qg_send, qg_recv, part_send, part_recv, tab_send, tab_recv,
    flood_sem, go_sem, relay_send,
):
    sp_size, tp_size = sizes
    total = sp_size * tp_size
    _, rows, features = qg_ref.shape
    heads, table_len = table_ref.shape
    head_dim = features // heads
    inv_root = head_dim ** -0.5
    table_width = tab.shape[1]
    sp, tp = lax.axis_index("sp"), lax.axis_index("tp")
    me = sp * tp_size + tp

    def device(index):
        return (index // tp_size, lax.rem(index, tp_size))

    stages = axis_stages(total)[::-1]

    group = stages[-1][1] if stages else 1
    inside = (lax.rem(me + 1, group) != 0) | (lax.rem((me + 1) // group, 2) == 1)
    sends = [None, (me >= 1) & (lax.rem(me, group) != 0), me >= 2]
    relays = (me + 2 < total) & (lax.rem(me + 2, group) == 0)

    def stage_place(stage):
        stride, factor = stage
        return lax.rem(me // stride, factor)

    def stage_peer(stage, place):
        return device(me + (place - stage_place(stage)) * stage[0])

    def columns(head):
        return pl.ds(pl.multiple_of(head * head_dim, head_dim), head_dim)

    first, others = pl.ds(0, head_dim), pl.ds(head_dim, features - head_dim)
    stat_rows = (pl.ds(0, heads), pl.ds(heads, heads))
    loads = [
        [(q_hbm.at[:, first], qg_ref.at[0, :, first]), (g_hbm.at[:, first], qg_ref.at[1, :, first])],
        [(log_hbm, rows_ref.at[stat_rows[0]]), (dot_hbm, rows_ref.at[stat_rows[1]])],
        [(q_hbm.at[:, others], qg_ref.at[0, :, others]), (g_hbm.at[:, others], qg_ref.at[1, :, others])],
        [(table_hbm, table_ref)],
        [(k_hbm, kv_ref.at[0]), (v_hbm, kv_ref.at[1])],
    ]
    loaded = [qg_ref.at[:, :, first], rows_ref, qg_ref.at[:, :, others], table_ref, kv_ref]

    def load_start(at):
        for source, target in loads[at]:
            pltpu.make_async_copy(source, target, load_sem.at[at]).start()

    def load_wait(at):
        pltpu.make_async_copy(loaded[at], loaded[at], load_sem.at[at]).wait()

    place = lax.rem(me, group)
    odd_group = lax.rem(me // group, 2) == 1
    held = jnp.where(place == 0, 1, jnp.where(place == 1, jnp.where(odd_group, 1, 3), jnp.where(place == 2, 1, 2)))
    barrier = pltpu.get_barrier_semaphore()
    for other, valid in (
        (me + 2, (me + 2 < total) & (place != group - 1)),
        (me + 1, me + 1 < total),
        (me - 1, lax.rem(place, 2) == 1),
    ):
        @pl.when(valid)
        def _():
            pl.semaphore_signal(barrier, inc=1, device_id=device(other), device_id_type=MESH)

    awaited = (me >= 1, (me >= 2) & (place != 1), (lax.rem(place, 2) == 0) & (me + 1 < total))
    count = sum(jnp.where(valid, 1, 0) for valid in awaited)

    for at in range(len(loads)):
        load_start(at)
    pl.semaphore_wait(barrier, count)

    def stat_copy(lag):
        return pltpu.make_async_remote_copy(
            src_ref=stat, dst_ref=stat_in.at[lag - 1],
            send_sem=stat_send.at[lag - 1], recv_sem=stat_recv.at[lag - 1],
            device_id=device(me - lag), device_id_type=MESH,
        )

    def qg_copy(lag, head):
        return pltpu.make_async_remote_copy(
            src_ref=qg_ref.at[:, :, columns(head)], dst_ref=qg_in.at[lag - 1, head],
            send_sem=qg_send.at[lag - 1], recv_sem=qg_recv.at[lag - 1, head],
            device_id=device(me - lag), device_id_type=MESH,
        )

    def relay_copy(head):
        return pltpu.make_async_remote_copy(
            src_ref=qg_in.at[1, head], dst_ref=qg_in.at[0, head],
            send_sem=relay_send.at[0], recv_sem=qg_recv.at[0, head],
            device_id=device(me + 1), device_id_type=MESH,
        )

    def relay(head):
        qg_copy(2, head).wait_recv()
        relay_copy(head).start()

    def part_copy(lag, head):
        return pltpu.make_async_remote_copy(
            src_ref=part_out.at[lag - 1, head], dst_ref=part_in.at[lag - 1, head],
            send_sem=part_send.at[lag - 1],
            recv_sem=part_recv.at[head if lag == 1 else heads],
            device_id=device(me + lag), device_id_type=MESH,
        )

    def whole(ref, send_sem, recv_sem):
        return pltpu.make_async_remote_copy(
            src_ref=ref, dst_ref=ref, send_sem=send_sem, recv_sem=recv_sem,
            device_id=device(me), device_id_type=MESH,
        )

    for which, source in enumerate((q_hbm, g_hbm)):
        @pl.when(sends[1])
        def _():
            pltpu.make_async_remote_copy(
                src_ref=source.at[:, first], dst_ref=qg_in.at[0, 0, which],
                send_sem=qg_send.at[0], recv_sem=qg_recv.at[0, 0],
                device_id=device(me - 1), device_id_type=MESH,
            ).start()

    @pl.when((place == 0) & (me >= 1))
    def _():
        pl.semaphore_signal(go_sem.at[0], inc=1, device_id=device(me + 1), device_id_type=MESH)

    @pl.when(sends[2] & (place != 1))
    def _():
        load_wait(0)
        qg_copy(2, 0).start()

    @pl.when(~(sends[2] & (place != 1)))
    def _():
        load_wait(0)

    load_wait(1)
    stat[0:heads, :] = rows_ref[0:heads, :] * LOG2E
    stat[heads:, :] = rows_ref[heads:, :]

    @pl.when(me >= 1)
    def _():
        stat_copy(1).start()

    load_wait(2)

    @pl.loop(1, heads)
    def _(head):
        @pl.when(sends[1])
        def _():
            qg_copy(1, head).start()

        @pl.when(sends[2] & (place != 1))
        def _():
            qg_copy(2, head).start()

    @pl.when(sends[2])
    def _():
        @pl.when(place == 1)
        def _():
            pl.semaphore_wait(go_sem.at[0], 1)

            @pl.loop(0, heads)
            def _(head):
                qg_copy(2, head).start()

        stat_copy(2).start()
        pl.semaphore_signal(flood_sem.at[0], inc=1, device_id=device(me - 2), device_id_type=MESH)

    reaches = flood_reaches(stages)

    def flood_others(at):
        others = (me + reaches[at], me - reaches[at])
        return [(other, (other >= 0) & (other < total)) for other in others]

    def flood_start(at):
        if at < len(reaches):
            for other, valid in flood_others(at):
                @pl.when(valid)
                def _():
                    pl.semaphore_signal(
                        flood_sem.at[at + 1], inc=1, device_id=device(other), device_id_type=MESH
                    )

    def flood_finish(at):
        if at < len(reaches):
            valid = [valid for _, valid in flood_others(at)]

            @pl.when(valid[0] | valid[1])
            def _():
                pl.semaphore_wait(
                    flood_sem.at[at + 1], sum(jnp.where(each, 1, 0) for each in valid)
                )

    load_wait(3)
    tab[...] = jnp.zeros_like(tab)
    tab[:, 0:table_len] = table_ref[...] * LOG2E
    padded = tab[...]
    from_zero = turn(padded, 1 - SEG_LEN)
    neg[...] = turn(padded, LANES - (SEG_LEN - 1))[:, 0:LANES]
    const[...] = jnp.broadcast_to(from_zero[:, rows:rows + 1], const.shape)
    tab[...] = from_zero
    key_at, query_at = iota((rows, rows), 0), iota((rows, rows), 1)
    edge[...] = jnp.where(query_at // SEG_LEN <= key_at // SEG_LEN, 0.0, MASKED)

    @pl.loop(0, heads)
    def _(head):
        row = jnp.broadcast_to(tab[pl.ds(head, 1), 0:rows], (SUBL, rows))
        near = sublane_turn(row, 1)
        row = jnp.broadcast_to(neg[pl.ds(head, 1), :], (SUBL, LANES))
        before = sublane_turn(row, 1)
        have = SUBL
        while have < rows:
            near = jnp.concatenate([near, turn(near, have)], axis=0)
            if have < LANES:
                before = jnp.concatenate([before, turn(before, have)], axis=0)
            have *= 2
        far = const[pl.ds(head, 1), :]
        upper = iota((rows, rows), 1) >= iota((rows, rows), 0)
        bias[1, head] = jnp.where(upper, far, near)
        segs_ok = iota((rows, rows), 1) // SEG_LEN >= iota((rows, rows), 0) // SEG_LEN
        wide = jnp.concatenate([before] * (rows // LANES), axis=1)
        tall = jnp.concatenate([wide] * (rows // LANES), axis=0)
        bias[0, head] = jnp.where(upper, near, jnp.where(segs_ok, tall, MASKED))

    def pair_terms(lag, head, queries, grads, log_row, dot_row):
        keys, values = kv_ref[0, :, columns(head)], kv_ref[1, :, columns(head)]
        across = (((1,), (1,)), ((), ()))
        scores = lax.dot_general(keys, queries, across, preferred_element_type=jnp.float32)
        if lag < 2:
            shift = bias[lag, head] - log_row
        else:
            shift = edge[...] + (const[pl.ds(head, 1), :] - log_row)
        weights = jnp.exp2(scores * (inv_root * LOG2E) + shift)
        weight_grads = lax.dot_general(values, grads, across, preferred_element_type=jnp.float32)
        score_grads = weights * (weight_grads - dot_row)
        score_grads_b = score_grads.astype(jnp.bfloat16)
        value_part = jnp.dot(
            weights.astype(jnp.bfloat16), grads, preferred_element_type=jnp.float32
        )
        key_part = jnp.dot(score_grads_b, queries, preferred_element_type=jnp.float32)
        query_part = lax.dot_general(
            score_grads_b, keys, (((0,), (0,)), ((), ())), preferred_element_type=jnp.float32
        )
        return score_grads, query_part, key_part, value_part

    load_wait(4)
    steps = len(reaches) + 1 if stages else 0
    in_loop = min(steps, heads // 2)

    def flood_step(at):
        if at == 0:
            @pl.when(me + 2 < total)
            def _():
                pl.semaphore_wait(flood_sem.at[0], 1)
        else:
            flood_finish(at - 1)
        flood_start(at)


    @pl.loop(0, heads)
    def _(head):
        score_grads, query_part, key_part, value_part = pair_terms(
            0, head, qg_ref[0, :, columns(head)], qg_ref[1, :, columns(head)],
            stat[pl.ds(head, 1), :], stat[pl.ds(head + heads, 1), :],
        )
        dq_own[head] = query_part
        dk_acc[head] = key_part
        dv_acc[head] = value_part
        upper = iota((rows, rows), 1) >= iota((rows, rows), 0)
        acc_pos[head] = fold_diagonals(jnp.where(upper, score_grads, 0.0))
        lower = jnp.where(upper, 0.0, score_grads)
        tiles = sum(
            lower[at:at + LANES, at:at + LANES] for at in range(0, rows, LANES)
        )
        acc_neg[head] = fold_diagonals(tiles)
        acc_const[head] = jnp.zeros(acc_const.shape[1:], jnp.float32)

        @pl.when(relays & (lax.rem(head, 2) == 1))
        def _():
            relay(head // 2)

        for at in range(in_loop):
            @pl.when(head == 2 * at + 1)
            def _():
                flood_step(at)

    def start_parts(first, last):
        @pl.loop(first, last)
        def _(head):
            part_copy(1, head).start()

    for at in range(in_loop, steps):
        flood_step(at)

    for lag in (2, 1):
        @pl.when(me + lag < total)
        def _():
            stat_copy(lag).wait_recv()

    @pl.loop(0, heads)
    def _(head):
        @pl.when(relays & (head < heads - heads // 2))
        def _():
            relay(head + heads // 2)

        for lag in (2, 1):
            @pl.when(me + lag < total)
            def _():
                @pl.when((lag == 1) | ~relays)
                def _():
                    qg_copy(lag, head).wait_recv()

                score_grads, query_part, key_part, value_part = pair_terms(
                    lag, head, qg_in[lag - 1, head, 0], qg_in[lag - 1, head, 1],
                    stat_in[lag - 1, pl.ds(head, 1), :],
                    stat_in[lag - 1, pl.ds(head + heads, 1), :],
                )
                part_out[lag - 1, head] = query_part.astype(jnp.bfloat16)
                if lag == 2:
                    part_copy(2, head).start()
                dk_acc[head] += key_part
                dv_acc[head] += value_part
                if lag == 1:
                    upper = iota((rows, rows), 1) >= iota((rows, rows), 0)
                    acc_const[head] += fold_rows(jnp.where(upper, score_grads, 0.0))
                    acc_pos[head] += fold_diagonals(jnp.where(upper, 0.0, score_grads))
                else:
                    acc_const[head] += fold_rows(score_grads)

        @pl.when((me + 1 < total) & inside & (head == heads - 2))
        def _():
            start_parts(0, heads - held)

        dk_ref[:, columns(head)] = (dk_acc[head] * inv_root).astype(dk_ref.dtype)
        dv_ref[:, columns(head)] = dv_acc[head].astype(dv_ref.dtype)
        near = jnp.sum(sublane_turn(acc_pos[head], -1), axis=0, keepdims=True)
        before = jnp.sum(sublane_turn(acc_neg[head], -1), axis=0, keepdims=True)
        far = jnp.sum(jnp.sum(acc_const[head], axis=0, keepdims=True), axis=1, keepdims=True)
        tail = jnp.broadcast_to(far, (1, table_width - rows))
        tail = jnp.where(iota(tail.shape, 1) == 0, tail, 0.0)
        here = iota(tab.shape, 0) == head
        tab[...] = jnp.where(here, jnp.concatenate([near, tail], axis=1), tab[...])
        neg[...] = jnp.where(iota(neg.shape, 0) == head, before, neg[...])

    spread = jnp.concatenate(
        [neg[...], jnp.zeros((heads, table_width - LANES), jnp.float32)], axis=1
    )
    running = turn(tab[...], SEG_LEN - 1) + turn(spread, -(LANES - (SEG_LEN - 1)))

    def tab_copy(at, place, peer_place):
        stage = stages[at]
        return pltpu.make_async_remote_copy(
            src_ref=tab_slots.at[at, place], dst_ref=tab_slots.at[at, place],
            send_sem=tab_send.at[at], recv_sem=tab_recv.at[at],
            device_id=stage_peer(stage, peer_place), device_id_type=MESH,
        )

    def stage_start(at, block):
        place = stage_place(stages[at])
        tab_slots[at, place] = block
        for offset in range(1, stages[at][1]):
            tab_copy(at, place, lax.rem(place + offset, stages[at][1])).start()

    def stage_finish(at):
        factor = stages[at][1]
        peers = tab_slots.at[at, pl.ds(0, factor - 1)]
        whole(peers, tab_send.at[at], tab_recv.at[at]).wait_recv()
        out = tab_slots[at, 0]
        for member in range(1, factor):
            out = out + tab_slots[at, member]
        return out

    if stages:
        stage_start(0, running)

    @pl.when((me + 1 < total) & ~inside)
    def _():
        start_parts(0, heads - held)

    for at in range(len(stages) - 1):
        stage_start(at + 1, stage_finish(at))

    @pl.when(me + 1 < total)
    def _():
        start_parts(heads - held, heads)

    @pl.when(me >= 2)
    def _():
        whole(part_in.at[1], part_send.at[1], part_recv.at[heads]).wait_recv()

        @pl.loop(0, heads)
        def _(head):
            dq_own[head] += part_in[1, head].astype(jnp.float32)

    @pl.loop(0, heads)
    def _(head):
        @pl.when(me >= 1)
        def _():
            part_copy(1, head).wait_recv()
            dq_own[head] += part_in[0, head].astype(jnp.float32)

        dq_ref[:, columns(head)] = (dq_own[head] * inv_root).astype(dq_ref.dtype)

    if stages:
        running = stage_finish(len(stages) - 1)
    dt_ref[...] = running[:, 0:table_len]

    for lag in (1, 2):
        @pl.when(me >= lag)
        def _():
            stat_copy(lag).wait_send()

        @pl.when(sends[lag])
        def _():
            whole(qg_ref, qg_send.at[lag - 1], qg_recv.at[lag - 1, 0]).wait_send()

        @pl.when(me + lag < total)
        def _():
            whole(part_out.at[lag - 1], part_send.at[lag - 1], part_recv.at[0]).wait_send()

    @pl.when(relays)
    def _():
        whole(qg_in.at[1], relay_send.at[0], qg_recv.at[0, 0]).wait_send()

    for at, (_, factor) in enumerate(stages):
        peers = tab_slots.at[at, pl.ds(0, factor - 1)]
        whole(peers, tab_send.at[at], tab_recv.at[at]).wait_send()


def store_kernel(*refs):
    sources, targets, sem = refs[:4], refs[4:8], refs[8]
    stores = [pltpu.make_async_copy(sources[at], targets[at], sem.at[at]) for at in range(4)]
    for store in stores:
        store.start()
    for store in stores:
        store.wait()


def local(sizes, query_rows, key_rows, value_rows, out_grad, log_totals, out_dot, bias_table):
    rows, features = query_rows.shape
    heads, table_len = bias_table.shape
    head_dim = features // heads
    assert LEFT_SEGS * SEG_LEN == 2 * rows and rows == REL_CLIP
    assert table_len == REL_CLIP + SEG_LEN and head_dim == LANES
    stage_list = axis_stages(sizes[0] * sizes[1])
    stage_count = max(len(stage_list), 1)
    flood_count = len(flood_reaches(stage_list)) + 1
    assert sizes[0] * sizes[1] % 4 == 0
    slot_count = max([factor for _, factor in stage_list] + [1])
    table_width = -(-(table_len + 1) // LANES) * LANES
    f32, bf16 = jnp.float32, jnp.bfloat16
    vmem = pl.BlockSpec(memory_space=pltpu.VMEM)
    dma = pltpu.SemaphoreType.DMA
    wide = pltpu.VMEM((rows, features), bf16)
    results = pl.pallas_call(
        functools.partial(kernel, sizes),
        out_shape=(wide, wide, wide, pltpu.VMEM((heads, table_len), f32)),
        in_specs=[pl.BlockSpec(memory_space=pltpu.HBM)] * 7,
        out_specs=(vmem,) * 4,
        scratch_shapes=[
            pltpu.VMEM((2, rows, features), bf16),
            pltpu.VMEM((2, rows, features), bf16),
            pltpu.VMEM((2 * heads, rows), f32),
            pltpu.VMEM((heads, table_len), f32),
            dma((5,)),
            pltpu.VMEM((2 * heads, rows), f32),
            pltpu.VMEM((2, 2 * heads, rows), f32),
            pltpu.VMEM((2, heads, 2, rows, head_dim), bf16),
            pltpu.VMEM((2, heads, rows, head_dim), bf16),
            pltpu.VMEM((2, heads, rows, head_dim), bf16),
            pltpu.VMEM((heads, rows, head_dim), f32),
            pltpu.VMEM((heads, rows, head_dim), f32),
            pltpu.VMEM((heads, rows, head_dim), f32),
            pltpu.VMEM((2, heads, rows, rows), f32),
            pltpu.VMEM((rows, rows), f32),
            pltpu.VMEM((heads, table_width), f32),
            pltpu.VMEM((heads, LANES), f32),
            pltpu.VMEM((heads, rows), f32),
            pltpu.VMEM((heads, SUBL, rows), f32),
            pltpu.VMEM((heads, SUBL, LANES), f32),
            pltpu.VMEM((heads, SUBL, rows), f32),
            pltpu.VMEM((stage_count, slot_count, heads, table_width), f32),
            dma((2,)), dma((2,)),
            dma((2,)), dma((2, heads)),
            dma((2,)), dma((heads + 1,)),
            dma((stage_count,)), dma((stage_count,)),
            pltpu.SemaphoreType.REGULAR((flood_count,)),
            pltpu.SemaphoreType.REGULAR((1,)), dma((1,)),
        ],
        compiler_params=pltpu.CompilerParams(
            collective_id=0, has_side_effects=True, vmem_limit_bytes=40 * 2**20
        ),
        name="band_backward",
    )(*(pltpu.with_memory_space_constraint(x, pltpu.HBM) for x in (query_rows, key_rows, value_rows, out_grad, log_totals.T, out_dot.T, bias_table)))
    return pl.pallas_call(
        store_kernel,
        out_shape=tuple(jax.ShapeDtypeStruct(x.shape, x.dtype) for x in results),
        in_specs=[vmem] * 4,
        out_specs=(pl.BlockSpec(memory_space=pltpu.HBM),) * 4,
        scratch_shapes=[dma((4,))],
        compiler_params=pltpu.CompilerParams(vmem_limit_bytes=2**20),
        name="store",
    )(*results)


def solution(mesh):
    sizes = (mesh.shape["sp"], mesh.shape["tp"])
    by_rows = P(("sp", "tp"), None)
    return jax.shard_map(
        functools.partial(local, sizes),
        mesh=mesh,
        in_specs=(by_rows,) * 6 + (P(),),
        out_specs=(by_rows, by_rows, by_rows, P()),
        check_vma=False,
    )
```

```python
import functools
import math

import jax
import jax.numpy as jnp
from jax import lax
from jax.experimental import pallas as pl
from jax.experimental.pallas import tpu as pltpu
from jax.sharding import PartitionSpec as P

SEG_LEN = 64
LEFT_SEGS = 8
REL_CLIP = 256
LANES = 128
SUBL = 8
MASKED = -1e30
LOG2E = math.log2(math.e)
MESH = pl.DeviceIdType.MESH


def axis_stages(size):
    stages, stride = [], 1
    while size > 1:
        order = (8, 4, 3, 2, 5, 7) if stages else (4, 3, 2, 5, 7)
        factor = next((f for f in order if size % f == 0), size)
        stages.append((stride, factor))
        stride *= factor
        size //= factor
    return stages


def flood_reaches(stages):
    reaches, reach = [], 2
    while reach < max([stride * (factor - 1) for stride, factor in stages] + [0]):
        reaches.append(reach)
        reach *= 2
    return reaches


def iota(shape, axis):
    return lax.broadcasted_iota(jnp.int32, shape, axis)


def turn(x, amount):
    width = x.shape[1]
    return pltpu.roll(x, amount % width, 1)


def fold_diagonals(x):
    rows = x.shape[0]
    while rows > SUBL:
        half = rows // 2
        x = x[:half] + turn(x[half:], -half)
        rows = half
    return x


def fold_rows(x):
    rows = x.shape[0]
    while rows > SUBL:
        half = rows // 2
        x = x[:half] + x[half:]
        rows = half
    return x


def sublane_turn(x, direction):
    subl = iota(x.shape, 0)
    for bit in (1, 2, 4):
        x = jnp.where((subl & bit) != 0, turn(x, direction * bit), x)
    return x


def kernel(
    sizes,
    q_hbm, k_hbm, v_hbm, g_hbm, log_hbm, dot_hbm, table_hbm,
    dq_ref, dk_ref, dv_ref, dt_ref,
    qg_ref, kv_ref, rows_ref, table_ref, load_sem,
    stat, stat_in, qg_in, part_out, part_in, dq_own, dk_acc, dv_acc,
    bias, edge, tab, neg, const, acc_pos, acc_neg, acc_const, tab_slots,
    stat_send, stat_recv, qg_send, qg_recv, part_send, part_recv, tab_send, tab_recv,
    flood_sem, go_sem, relay_send,
):
    sp_size, tp_size = sizes
    total = sp_size * tp_size
    _, rows, features = qg_ref.shape
    heads, table_len = table_ref.shape
    head_dim = features // heads
    inv_root = head_dim ** -0.5
    table_width = tab.shape[1]
    sp, tp = lax.axis_index("sp"), lax.axis_index("tp")
    me = sp * tp_size + tp

    def device(index):
        return (index // tp_size, lax.rem(index, tp_size))

    stages = axis_stages(total)[::-1]

    group = stages[-1][1] if stages else 1
    inside = (lax.rem(me + 1, group) != 0) | (lax.rem((me + 1) // group, 2) == 1)
    sends = [None, (me >= 1) & (lax.rem(me, group) != 0), me >= 2]
    relays = (me + 2 < total) & (lax.rem(me + 2, group) == 0)

    def stage_place(stage):
        stride, factor = stage
        return lax.rem(me // stride, factor)

    def stage_peer(stage, place):
        return device(me + (place - stage_place(stage)) * stage[0])

    def columns(head):
        return pl.ds(pl.multiple_of(head * head_dim, head_dim), head_dim)

    first, others = pl.ds(0, head_dim), pl.ds(head_dim, features - head_dim)
    stat_rows = (pl.ds(0, heads), pl.ds(heads, heads))
    loads = [
        [(q_hbm.at[:, first], qg_ref.at[0, :, first]), (g_hbm.at[:, first], qg_ref.at[1, :, first])],
        [(log_hbm, rows_ref.at[stat_rows[0]]), (dot_hbm, rows_ref.at[stat_rows[1]])],
        [(q_hbm.at[:, others], qg_ref.at[0, :, others]), (g_hbm.at[:, others], qg_ref.at[1, :, others])],
        [(table_hbm, table_ref)],
        [(k_hbm, kv_ref.at[0]), (v_hbm, kv_ref.at[1])],
    ]
    loaded = [qg_ref.at[:, :, first], rows_ref, qg_ref.at[:, :, others], table_ref, kv_ref]

    def load_start(at):
        for source, target in loads[at]:
            pltpu.make_async_copy(source, target, load_sem.at[at]).start()

    def load_wait(at):
        pltpu.make_async_copy(loaded[at], loaded[at], load_sem.at[at]).wait()

    place = lax.rem(me, group)
    held = min(2, heads)
    barrier = pltpu.get_barrier_semaphore()
    for other, valid in (
        (me + 2, (me + 2 < total) & (place != group - 1)),
        (me + 1, me + 1 < total),
        (me - 1, lax.rem(place, 2) == 1),
    ):
        @pl.when(valid)
        def _():
            pl.semaphore_signal(barrier, inc=1, device_id=device(other), device_id_type=MESH)

    awaited = (me >= 1, (me >= 2) & (place != 1), (lax.rem(place, 2) == 0) & (me + 1 < total))
    count = sum(jnp.where(valid, 1, 0) for valid in awaited)

    for at in range(len(loads)):
        load_start(at)
    pl.semaphore_wait(barrier, count)

    def stat_copy(lag):
        return pltpu.make_async_remote_copy(
            src_ref=stat, dst_ref=stat_in.at[lag - 1],
            send_sem=stat_send.at[lag - 1], recv_sem=stat_recv.at[lag - 1],
            device_id=device(me - lag), device_id_type=MESH,
        )

    def qg_copy(lag, head):
        return pltpu.make_async_remote_copy(
            src_ref=qg_ref.at[:, :, columns(head)], dst_ref=qg_in.at[lag - 1, head],
            send_sem=qg_send.at[lag - 1], recv_sem=qg_recv.at[lag - 1, head],
            device_id=device(me - lag), device_id_type=MESH,
        )

    def relay_copy(head):
        return pltpu.make_async_remote_copy(
            src_ref=qg_in.at[1, head], dst_ref=qg_in.at[0, head],
            send_sem=relay_send.at[0], recv_sem=qg_recv.at[0, head],
            device_id=device(me + 1), device_id_type=MESH,
        )

    def relay(head):
        qg_copy(2, head).wait_recv()
        relay_copy(head).start()

    def part_copy(lag, head):
        return pltpu.make_async_remote_copy(
            src_ref=part_out.at[lag - 1, head], dst_ref=part_in.at[lag - 1, head],
            send_sem=part_send.at[lag - 1],
            recv_sem=part_recv.at[head if lag == 1 else heads],
            device_id=device(me + lag), device_id_type=MESH,
        )

    def whole(ref, send_sem, recv_sem):
        return pltpu.make_async_remote_copy(
            src_ref=ref, dst_ref=ref, send_sem=send_sem, recv_sem=recv_sem,
            device_id=device(me), device_id_type=MESH,
        )

    for which, source in enumerate((q_hbm, g_hbm)):
        @pl.when(sends[1])
        def _():
            pltpu.make_async_remote_copy(
                src_ref=source.at[:, first], dst_ref=qg_in.at[0, 0, which],
                send_sem=qg_send.at[0], recv_sem=qg_recv.at[0, 0],
                device_id=device(me - 1), device_id_type=MESH,
            ).start()

    @pl.when((place == 0) & (me >= 1))
    def _():
        pl.semaphore_signal(go_sem.at[0], inc=1, device_id=device(me + 1), device_id_type=MESH)

    @pl.when(sends[2] & (place != 1))
    def _():
        load_wait(0)
        qg_copy(2, 0).start()

    @pl.when(~(sends[2] & (place != 1)))
    def _():
        load_wait(0)

    load_wait(1)
    stat[0:heads, :] = rows_ref[0:heads, :] * LOG2E
    stat[heads:, :] = rows_ref[heads:, :]

    @pl.when(me >= 1)
    def _():
        stat_copy(1).start()

    @pl.when(sends[2] & (place != 1))
    def _():
        stat_copy(2).start()

    load_wait(2)

    @pl.loop(1, heads)
    def _(head):
        @pl.when(sends[1])
        def _():
            qg_copy(1, head).start()

        @pl.when(sends[2] & (place != 1))
        def _():
            qg_copy(2, head).start()

    @pl.when(sends[2])
    def _():
        @pl.when(place == 1)
        def _():
            pl.semaphore_wait(go_sem.at[0], 1)
            stat_copy(2).start()

            @pl.loop(0, heads)
            def _(head):
                qg_copy(2, head).start()

        pl.semaphore_signal(flood_sem.at[0], inc=1, device_id=device(me - 2), device_id_type=MESH)

    reaches = flood_reaches(stages)

    def flood_others(at):
        others = (me + reaches[at], me - reaches[at])
        return [(other, (other >= 0) & (other < total)) for other in others]

    def flood_start(at):
        if at < len(reaches):
            for other, valid in flood_others(at):
                @pl.when(valid)
                def _():
                    pl.semaphore_signal(
                        flood_sem.at[at + 1], inc=1, device_id=device(other), device_id_type=MESH
                    )

    def flood_finish(at):
        if at < len(reaches):
            valid = [valid for _, valid in flood_others(at)]

            @pl.when(valid[0] | valid[1])
            def _():
                pl.semaphore_wait(
                    flood_sem.at[at + 1], sum(jnp.where(each, 1, 0) for each in valid)
                )

    load_wait(3)
    tab[...] = jnp.zeros_like(tab)
    tab[:, 0:table_len] = table_ref[...] * LOG2E
    padded = tab[...]
    from_zero = turn(padded, 1 - SEG_LEN)
    neg[...] = turn(padded, LANES - (SEG_LEN - 1))[:, 0:LANES]
    const[...] = jnp.broadcast_to(from_zero[:, rows:rows + 1], const.shape)
    tab[...] = from_zero
    key_at, query_at = iota((rows, rows), 0), iota((rows, rows), 1)
    edge[...] = jnp.where(query_at // SEG_LEN <= key_at // SEG_LEN, 0.0, MASKED)

    @pl.loop(0, heads)
    def _(head):
        row = jnp.broadcast_to(tab[pl.ds(head, 1), 0:rows], (SUBL, rows))
        near = sublane_turn(row, 1)
        row = jnp.broadcast_to(neg[pl.ds(head, 1), :], (SUBL, LANES))
        before = sublane_turn(row, 1)
        have = SUBL
        while have < rows:
            near = jnp.concatenate([near, turn(near, have)], axis=0)
            if have < LANES:
                before = jnp.concatenate([before, turn(before, have)], axis=0)
            have *= 2
        far = const[pl.ds(head, 1), :]
        upper = iota((rows, rows), 1) >= iota((rows, rows), 0)
        bias[1, head] = jnp.where(upper, far, near)
        segs_ok = iota((rows, rows), 1) // SEG_LEN >= iota((rows, rows), 0) // SEG_LEN
        wide = jnp.concatenate([before] * (rows // LANES), axis=1)
        tall = jnp.concatenate([wide] * (rows // LANES), axis=0)
        bias[0, head] = jnp.where(upper, near, jnp.where(segs_ok, tall, MASKED))

    def pair_terms(lag, head, queries, grads, log_row, dot_row):
        keys, values = kv_ref[0, :, columns(head)], kv_ref[1, :, columns(head)]
        across = (((1,), (1,)), ((), ()))
        scores = lax.dot_general(keys, queries, across, preferred_element_type=jnp.float32)
        if lag < 2:
            shift = bias[lag, head] - log_row
        else:
            shift = edge[...] + (const[pl.ds(head, 1), :] - log_row)
        weights = jnp.exp2(scores * (inv_root * LOG2E) + shift)
        weight_grads = lax.dot_general(values, grads, across, preferred_element_type=jnp.float32)
        score_grads = weights * (weight_grads - dot_row)
        score_grads_b = score_grads.astype(jnp.bfloat16)
        value_part = jnp.dot(
            weights.astype(jnp.bfloat16), grads, preferred_element_type=jnp.float32
        )
        key_part = jnp.dot(score_grads_b, queries, preferred_element_type=jnp.float32)
        query_part = lax.dot_general(
            score_grads_b, keys, (((0,), (0,)), ((), ())), preferred_element_type=jnp.float32
        )
        return score_grads, query_part, key_part, value_part

    load_wait(4)
    steps = len(reaches) + 1 if stages else 0
    in_loop = min(steps, heads // 2)

    def flood_step(at):
        if at == 0:
            @pl.when(me + 2 < total)
            def _():
                pl.semaphore_wait(flood_sem.at[0], 1)
        else:
            flood_finish(at - 1)
        flood_start(at)


    @pl.loop(0, heads)
    def _(head):
        score_grads, query_part, key_part, value_part = pair_terms(
            0, head, qg_ref[0, :, columns(head)], qg_ref[1, :, columns(head)],
            stat[pl.ds(head, 1), :], stat[pl.ds(head + heads, 1), :],
        )
        dq_own[head] = query_part
        dk_acc[head] = key_part
        dv_acc[head] = value_part
        upper = iota((rows, rows), 1) >= iota((rows, rows), 0)
        acc_pos[head] = fold_diagonals(jnp.where(upper, score_grads, 0.0))
        lower = jnp.where(upper, 0.0, score_grads)
        tiles = sum(
            lower[at:at + LANES, at:at + LANES] for at in range(0, rows, LANES)
        )
        acc_neg[head] = fold_diagonals(tiles)
        acc_const[head] = jnp.zeros(acc_const.shape[1:], jnp.float32)

        @pl.when(relays & (lax.rem(head, 2) == 1))
        def _():
            relay(head // 2)

        for at in range(in_loop):
            @pl.when(head == 2 * at + 1)
            def _():
                flood_step(at)

    def start_parts(first, last):
        @pl.loop(first, last)
        def _(head):
            part_copy(1, head).start()

    for at in range(in_loop, steps):
        flood_step(at)

    for lag in (2, 1):
        @pl.when(me + lag < total)
        def _():
            stat_copy(lag).wait_recv()

    @pl.loop(0, heads)
    def _(head):
        @pl.when(relays & (head < heads - heads // 2))
        def _():
            relay(head + heads // 2)

        for lag in (2, 1):
            @pl.when(me + lag < total)
            def _():
                @pl.when((lag == 1) | ~relays)
                def _():
                    qg_copy(lag, head).wait_recv()

                score_grads, query_part, key_part, value_part = pair_terms(
                    lag, head, qg_in[lag - 1, head, 0], qg_in[lag - 1, head, 1],
                    stat_in[lag - 1, pl.ds(head, 1), :],
                    stat_in[lag - 1, pl.ds(head + heads, 1), :],
                )
                part_out[lag - 1, head] = query_part.astype(jnp.bfloat16)
                if lag == 2:
                    part_copy(2, head).start()
                dk_acc[head] += key_part
                dv_acc[head] += value_part
                if lag == 1:
                    upper = iota((rows, rows), 1) >= iota((rows, rows), 0)
                    acc_const[head] += fold_rows(jnp.where(upper, score_grads, 0.0))
                    acc_pos[head] += fold_diagonals(jnp.where(upper, 0.0, score_grads))
                else:
                    acc_const[head] += fold_rows(score_grads)

        @pl.when((me + 1 < total) & inside & (head == heads - 2))
        def _():
            start_parts(0, heads - held)

        dk_ref[:, columns(head)] = (dk_acc[head] * inv_root).astype(dk_ref.dtype)
        dv_ref[:, columns(head)] = dv_acc[head].astype(dv_ref.dtype)
        near = jnp.sum(sublane_turn(acc_pos[head], -1), axis=0, keepdims=True)
        before = jnp.sum(sublane_turn(acc_neg[head], -1), axis=0, keepdims=True)
        far = jnp.sum(jnp.sum(acc_const[head], axis=0, keepdims=True), axis=1, keepdims=True)
        tail = jnp.broadcast_to(far, (1, table_width - rows))
        tail = jnp.where(iota(tail.shape, 1) == 0, tail, 0.0)
        here = iota(tab.shape, 0) == head
        tab[...] = jnp.where(here, jnp.concatenate([near, tail], axis=1), tab[...])
        neg[...] = jnp.where(iota(neg.shape, 0) == head, before, neg[...])

    spread = jnp.concatenate(
        [neg[...], jnp.zeros((heads, table_width - LANES), jnp.float32)], axis=1
    )
    running = turn(tab[...], SEG_LEN - 1) + turn(spread, -(LANES - (SEG_LEN - 1)))

    def tab_copy(at, place, peer_place):
        stage = stages[at]
        return pltpu.make_async_remote_copy(
            src_ref=tab_slots.at[at, place], dst_ref=tab_slots.at[at, place],
            send_sem=tab_send.at[at], recv_sem=tab_recv.at[at],
            device_id=stage_peer(stage, peer_place), device_id_type=MESH,
        )

    def stage_start(at, block):
        place = stage_place(stages[at])
        tab_slots[at, place] = block
        for offset in range(1, stages[at][1]):
            tab_copy(at, place, lax.rem(place + offset, stages[at][1])).start()

    def stage_finish(at):
        factor = stages[at][1]
        peers = tab_slots.at[at, pl.ds(0, factor - 1)]
        whole(peers, tab_send.at[at], tab_recv.at[at]).wait_recv()
        out = tab_slots[at, 0]
        for member in range(1, factor):
            out = out + tab_slots[at, member]
        return out

    if stages:
        stage_start(0, running)

    @pl.when((me + 1 < total) & ~inside)
    def _():
        start_parts(0, heads - held)

    for at in range(len(stages) - 1):
        stage_start(at + 1, stage_finish(at))

    @pl.when(me + 1 < total)
    def _():
        start_parts(heads - held, heads)

    @pl.when(me >= 2)
    def _():
        whole(part_in.at[1], part_send.at[1], part_recv.at[heads]).wait_recv()

        @pl.loop(0, heads)
        def _(head):
            dq_own[head] += part_in[1, head].astype(jnp.float32)

    @pl.loop(0, heads)
    def _(head):
        @pl.when(me >= 1)
        def _():
            part_copy(1, head).wait_recv()
            dq_own[head] += part_in[0, head].astype(jnp.float32)

        dq_ref[:, columns(head)] = (dq_own[head] * inv_root).astype(dq_ref.dtype)

    if stages:
        running = stage_finish(len(stages) - 1)
    dt_ref[...] = running[:, 0:table_len]

    for lag in (1, 2):
        @pl.when(me >= lag)
        def _():
            stat_copy(lag).wait_send()

        @pl.when(sends[lag])
        def _():
            whole(qg_ref, qg_send.at[lag - 1], qg_recv.at[lag - 1, 0]).wait_send()

        @pl.when(me + lag < total)
        def _():
            whole(part_out.at[lag - 1], part_send.at[lag - 1], part_recv.at[0]).wait_send()

    @pl.when(relays)
    def _():
        whole(qg_in.at[1], relay_send.at[0], qg_recv.at[0, 0]).wait_send()

    for at, (_, factor) in enumerate(stages):
        peers = tab_slots.at[at, pl.ds(0, factor - 1)]
        whole(peers, tab_send.at[at], tab_recv.at[at]).wait_send()


def store_kernel(*refs):
    sources, targets, sem = refs[:4], refs[4:8], refs[8]
    stores = [pltpu.make_async_copy(sources[at], targets[at], sem.at[at]) for at in range(4)]
    for store in stores:
        store.start()
    for store in stores:
        store.wait()


def local(sizes, query_rows, key_rows, value_rows, out_grad, log_totals, out_dot, bias_table):
    rows, features = query_rows.shape
    heads, table_len = bias_table.shape
    head_dim = features // heads
    assert LEFT_SEGS * SEG_LEN == 2 * rows and rows == REL_CLIP
    assert table_len == REL_CLIP + SEG_LEN and head_dim == LANES
    stage_list = axis_stages(sizes[0] * sizes[1])
    stage_count = max(len(stage_list), 1)
    flood_count = len(flood_reaches(stage_list)) + 1
    assert sizes[0] * sizes[1] % 4 == 0
    slot_count = max([factor for _, factor in stage_list] + [1])
    table_width = -(-(table_len + 1) // LANES) * LANES
    f32, bf16 = jnp.float32, jnp.bfloat16
    vmem = pl.BlockSpec(memory_space=pltpu.VMEM)
    dma = pltpu.SemaphoreType.DMA
    wide = pltpu.VMEM((rows, features), bf16)
    results = pl.pallas_call(
        functools.partial(kernel, sizes),
        out_shape=(wide, wide, wide, pltpu.VMEM((heads, table_len), f32)),
        in_specs=[pl.BlockSpec(memory_space=pltpu.HBM)] * 7,
        out_specs=(vmem,) * 4,
        scratch_shapes=[
            pltpu.VMEM((2, rows, features), bf16),
            pltpu.VMEM((2, rows, features), bf16),
            pltpu.VMEM((2 * heads, rows), f32),
            pltpu.VMEM((heads, table_len), f32),
            dma((5,)),
            pltpu.VMEM((2 * heads, rows), f32),
            pltpu.VMEM((2, 2 * heads, rows), f32),
            pltpu.VMEM((2, heads, 2, rows, head_dim), bf16),
            pltpu.VMEM((2, heads, rows, head_dim), bf16),
            pltpu.VMEM((2, heads, rows, head_dim), bf16),
            pltpu.VMEM((heads, rows, head_dim), f32),
            pltpu.VMEM((heads, rows, head_dim), f32),
            pltpu.VMEM((heads, rows, head_dim), f32),
            pltpu.VMEM((2, heads, rows, rows), f32),
            pltpu.VMEM((rows, rows), f32),
            pltpu.VMEM((heads, table_width), f32),
            pltpu.VMEM((heads, LANES), f32),
            pltpu.VMEM((heads, rows), f32),
            pltpu.VMEM((heads, SUBL, rows), f32),
            pltpu.VMEM((heads, SUBL, LANES), f32),
            pltpu.VMEM((heads, SUBL, rows), f32),
            pltpu.VMEM((stage_count, slot_count, heads, table_width), f32),
            dma((2,)), dma((2,)),
            dma((2,)), dma((2, heads)),
            dma((2,)), dma((heads + 1,)),
            dma((stage_count,)), dma((stage_count,)),
            pltpu.SemaphoreType.REGULAR((flood_count,)),
            pltpu.SemaphoreType.REGULAR((1,)), dma((1,)),
        ],
        compiler_params=pltpu.CompilerParams(
            collective_id=0, has_side_effects=True, vmem_limit_bytes=40 * 2**20
        ),
        name="band_backward",
    )(*(pltpu.with_memory_space_constraint(x, pltpu.HBM) for x in (query_rows, key_rows, value_rows, out_grad, log_totals.T, out_dot.T, bias_table)))
    return pl.pallas_call(
        store_kernel,
        out_shape=tuple(jax.ShapeDtypeStruct(x.shape, x.dtype) for x in results),
        in_specs=[vmem] * 4,
        out_specs=(pl.BlockSpec(memory_space=pltpu.HBM),) * 4,
        scratch_shapes=[dma((4,))],
        compiler_params=pltpu.CompilerParams(vmem_limit_bytes=2**20),
        name="store",
    )(*results)


def solution(mesh):
    sizes = (mesh.shape["sp"], mesh.shape["tp"])
    by_rows = P(("sp", "tp"), None)
    return jax.shard_map(
        functools.partial(local, sizes),
        mesh=mesh,
        in_specs=(by_rows,) * 6 + (P(),),
        out_specs=(by_rows, by_rows, by_rows, P()),
        check_vma=False,
    )
```

```python
import functools
import math

import jax
import jax.numpy as jnp
from jax import lax
from jax.experimental import pallas as pl
from jax.experimental.pallas import tpu as pltpu
from jax.sharding import PartitionSpec as P

SEG_LEN = 64
LEFT_SEGS = 8
REL_CLIP = 256
LANES = 128
SUBL = 8
MASKED = -1e30
LOG2E = math.log2(math.e)
MESH = pl.DeviceIdType.MESH


def axis_stages(size):
    stages, stride = [], 1
    while size > 1:
        order = (8, 4, 3, 2, 5, 7) if stages else (4, 3, 2, 5, 7)
        factor = next((f for f in order if size % f == 0), size)
        stages.append((stride, factor))
        stride *= factor
        size //= factor
    return stages


def flood_reaches(stages):
    reaches, reach = [], 2
    while reach < max([stride * (factor - 1) for stride, factor in stages] + [0]):
        reaches.append(reach)
        reach *= 2
    return reaches


def iota(shape, axis):
    return lax.broadcasted_iota(jnp.int32, shape, axis)


def turn(x, amount):
    width = x.shape[1]
    return pltpu.roll(x, amount % width, 1)


def fold_diagonals(x):
    rows = x.shape[0]
    while rows > SUBL:
        half = rows // 2
        x = x[:half] + turn(x[half:], -half)
        rows = half
    return x


def fold_rows(x):
    rows = x.shape[0]
    while rows > SUBL:
        half = rows // 2
        x = x[:half] + x[half:]
        rows = half
    return x


def sublane_turn(x, direction):
    subl = iota(x.shape, 0)
    for bit in (1, 2, 4):
        x = jnp.where((subl & bit) != 0, turn(x, direction * bit), x)
    return x


def kernel(
    sizes,
    q_hbm, k_hbm, v_hbm, g_hbm, log_hbm, dot_hbm, table_hbm,
    dq_ref, dk_ref, dv_ref, dt_ref,
    qg_ref, kv_ref, rows_ref, table_ref, load_sem,
    stat, stat_in, qg_in, part_out, part_in, dq_own, dk_acc, dv_acc,
    bias, edge, tab, neg, const, acc_pos, acc_neg, acc_const, tab_slots,
    stat_send, stat_recv, qg_send, qg_recv, part_send, part_recv, tab_send, tab_recv,
    flood_sem, go_sem, relay_send, detour_in, detour_send, detour_recv,
):
    sp_size, tp_size = sizes
    total = sp_size * tp_size
    _, rows, features = qg_ref.shape
    heads, table_len = table_ref.shape
    head_dim = features // heads
    inv_root = head_dim ** -0.5
    table_width = tab.shape[1]
    sp, tp = lax.axis_index("sp"), lax.axis_index("tp")
    me = sp * tp_size + tp

    def device(index):
        return (index // tp_size, lax.rem(index, tp_size))

    stages = axis_stages(total)[::-1]

    group = stages[-1][1] if stages else 1
    inside = (lax.rem(me + 1, group) != 0) | (lax.rem((me + 1) // group, 2) == 1)
    sends = [None, (me >= 1) & (lax.rem(me, group) != 0), me >= 2]
    relays = (me + 2 < total) & (lax.rem(me + 2, group) == 0)

    def stage_place(stage):
        stride, factor = stage
        return lax.rem(me // stride, factor)

    def stage_peer(stage, place):
        return device(me + (place - stage_place(stage)) * stage[0])

    def columns(head):
        return pl.ds(pl.multiple_of(head * head_dim, head_dim), head_dim)

    first, others = pl.ds(0, head_dim), pl.ds(head_dim, features - head_dim)
    stat_rows = (pl.ds(0, heads), pl.ds(heads, heads))
    loads = [
        [(q_hbm.at[:, first], qg_ref.at[0, :, first]), (g_hbm.at[:, first], qg_ref.at[1, :, first])],
        [(log_hbm, rows_ref.at[stat_rows[0]]), (dot_hbm, rows_ref.at[stat_rows[1]])],
        [(q_hbm.at[:, others], qg_ref.at[0, :, others]), (g_hbm.at[:, others], qg_ref.at[1, :, others])],
        [(table_hbm, table_ref)],
        [(k_hbm, kv_ref.at[0]), (v_hbm, kv_ref.at[1])],
    ]
    loaded = [qg_ref.at[:, :, first], rows_ref, qg_ref.at[:, :, others], table_ref, kv_ref]

    def load_start(at):
        for source, target in loads[at]:
            pltpu.make_async_copy(source, target, load_sem.at[at]).start()

    def load_wait(at):
        pltpu.make_async_copy(loaded[at], loaded[at], load_sem.at[at]).wait()

    place = lax.rem(me, group)
    held = jnp.where(place == 0, 1, jnp.where(place == 1, jnp.where(lax.rem(me // group, 2) == 1, 1, 2), 2))
    barrier = pltpu.get_barrier_semaphore()
    for other, valid in (
        (me + 2, (me + 2 < total) & (place != group - 1)),
        (me + 1, me + 1 < total),
        (me - 1, lax.rem(place, 2) == 1),
    ):
        @pl.when(valid)
        def _():
            pl.semaphore_signal(barrier, inc=1, device_id=device(other), device_id_type=MESH)

    awaited = (me >= 1, (me >= 2) & (place != 1), (lax.rem(place, 2) == 0) & (me + 1 < total))
    count = sum(jnp.where(valid, 1, 0) for valid in awaited)

    for at in range(len(loads)):
        load_start(at)
    pl.semaphore_wait(barrier, count)

    def stat_copy(lag):
        return pltpu.make_async_remote_copy(
            src_ref=stat, dst_ref=stat_in.at[lag - 1],
            send_sem=stat_send.at[lag - 1], recv_sem=stat_recv.at[lag - 1],
            device_id=device(me - lag), device_id_type=MESH,
        )

    def qg_copy(lag, head):
        return pltpu.make_async_remote_copy(
            src_ref=qg_ref.at[:, :, columns(head)], dst_ref=qg_in.at[lag - 1, head],
            send_sem=qg_send.at[lag - 1], recv_sem=qg_recv.at[lag - 1, head],
            device_id=device(me - lag), device_id_type=MESH,
        )

    def relay_copy(head):
        return pltpu.make_async_remote_copy(
            src_ref=qg_in.at[1, head], dst_ref=qg_in.at[0, head],
            send_sem=relay_send.at[0], recv_sem=qg_recv.at[0, head],
            device_id=device(me + 1), device_id_type=MESH,
        )

    def relay(head):
        qg_copy(2, head).wait_recv()
        relay_copy(head).start()

    def part_copy(lag, head):
        return pltpu.make_async_remote_copy(
            src_ref=part_out.at[lag - 1, head], dst_ref=part_in.at[lag - 1, head],
            send_sem=part_send.at[lag - 1],
            recv_sem=part_recv.at[head if lag == 1 else heads],
            device_id=device(me + lag), device_id_type=MESH,
        )

    def whole(ref, send_sem, recv_sem):
        return pltpu.make_async_remote_copy(
            src_ref=ref, dst_ref=ref, send_sem=send_sem, recv_sem=recv_sem,
            device_id=device(me), device_id_type=MESH,
        )

    for which, source in enumerate((q_hbm, g_hbm)):
        @pl.when(sends[1])
        def _():
            pltpu.make_async_remote_copy(
                src_ref=source.at[:, first], dst_ref=qg_in.at[0, 0, which],
                send_sem=qg_send.at[0], recv_sem=qg_recv.at[0, 0],
                device_id=device(me - 1), device_id_type=MESH,
            ).start()

    @pl.when((place == 0) & (me >= 1))
    def _():
        pl.semaphore_signal(go_sem.at[0], inc=1, device_id=device(me + 1), device_id_type=MESH)

    @pl.when(sends[2] & (place != 1))
    def _():
        load_wait(0)
        qg_copy(2, 0).start()

    @pl.when(~(sends[2] & (place != 1)))
    def _():
        load_wait(0)

    load_wait(1)
    stat[0:heads, :] = rows_ref[0:heads, :] * LOG2E
    stat[heads:, :] = rows_ref[heads:, :]

    @pl.when(me >= 1)
    def _():
        stat_copy(1).start()

    @pl.when(sends[2] & (place != 1))
    def _():
        stat_copy(2).start()

    load_wait(2)

    @pl.loop(1, heads)
    def _(head):
        @pl.when(sends[1])
        def _():
            qg_copy(1, head).start()

        @pl.when(sends[2] & (place != 1))
        def _():
            qg_copy(2, head).start()

    @pl.when(sends[2])
    def _():
        @pl.when(place == 1)
        def _():
            pl.semaphore_wait(go_sem.at[0], 1)
            stat_copy(2).start()

            @pl.loop(0, heads)
            def _(head):
                qg_copy(2, head).start()

        pl.semaphore_signal(flood_sem.at[0], inc=1, device_id=device(me - 2), device_id_type=MESH)

    reaches = flood_reaches(stages)

    def flood_others(at):
        others = (me + reaches[at], me - reaches[at])
        return [(other, (other >= 0) & (other < total)) for other in others]

    def flood_start(at):
        if at < len(reaches):
            for other, valid in flood_others(at):
                @pl.when(valid)
                def _():
                    pl.semaphore_signal(
                        flood_sem.at[at + 1], inc=1, device_id=device(other), device_id_type=MESH
                    )

    def flood_finish(at):
        if at < len(reaches):
            valid = [valid for _, valid in flood_others(at)]

            @pl.when(valid[0] | valid[1])
            def _():
                pl.semaphore_wait(
                    flood_sem.at[at + 1], sum(jnp.where(each, 1, 0) for each in valid)
                )

    load_wait(3)
    tab[...] = jnp.zeros_like(tab)
    tab[:, 0:table_len] = table_ref[...] * LOG2E
    padded = tab[...]
    from_zero = turn(padded, 1 - SEG_LEN)
    neg[...] = turn(padded, LANES - (SEG_LEN - 1))[:, 0:LANES]
    const[...] = jnp.broadcast_to(from_zero[:, rows:rows + 1], const.shape)
    tab[...] = from_zero
    key_at, query_at = iota((rows, rows), 0), iota((rows, rows), 1)
    edge[...] = jnp.where(query_at // SEG_LEN <= key_at // SEG_LEN, 0.0, MASKED)

    @pl.loop(0, heads)
    def _(head):
        row = jnp.broadcast_to(tab[pl.ds(head, 1), 0:rows], (SUBL, rows))
        near = sublane_turn(row, 1)
        row = jnp.broadcast_to(neg[pl.ds(head, 1), :], (SUBL, LANES))
        before = sublane_turn(row, 1)
        have = SUBL
        while have < rows:
            near = jnp.concatenate([near, turn(near, have)], axis=0)
            if have < LANES:
                before = jnp.concatenate([before, turn(before, have)], axis=0)
            have *= 2
        far = const[pl.ds(head, 1), :]
        upper = iota((rows, rows), 1) >= iota((rows, rows), 0)
        bias[1, head] = jnp.where(upper, far, near)
        segs_ok = iota((rows, rows), 1) // SEG_LEN >= iota((rows, rows), 0) // SEG_LEN
        wide = jnp.concatenate([before] * (rows // LANES), axis=1)
        tall = jnp.concatenate([wide] * (rows // LANES), axis=0)
        bias[0, head] = jnp.where(upper, near, jnp.where(segs_ok, tall, MASKED))

    def pair_terms(lag, head, queries, grads, log_row, dot_row):
        keys, values = kv_ref[0, :, columns(head)], kv_ref[1, :, columns(head)]
        across = (((1,), (1,)), ((), ()))
        scores = lax.dot_general(keys, queries, across, preferred_element_type=jnp.float32)
        if lag < 2:
            shift = bias[lag, head] - log_row
        else:
            shift = edge[...] + (const[pl.ds(head, 1), :] - log_row)
        weights = jnp.exp2(scores * (inv_root * LOG2E) + shift)
        weight_grads = lax.dot_general(values, grads, across, preferred_element_type=jnp.float32)
        score_grads = weights * (weight_grads - dot_row)
        score_grads_b = score_grads.astype(jnp.bfloat16)
        value_part = jnp.dot(
            weights.astype(jnp.bfloat16), grads, preferred_element_type=jnp.float32
        )
        key_part = jnp.dot(score_grads_b, queries, preferred_element_type=jnp.float32)
        query_part = lax.dot_general(
            score_grads_b, keys, (((0,), (0,)), ((), ())), preferred_element_type=jnp.float32
        )
        return score_grads, query_part, key_part, value_part

    load_wait(4)
    steps = len(reaches) + 1 if stages else 0
    in_loop = min(steps, heads // 2)

    def flood_step(at):
        if at == 0:
            @pl.when(me + 2 < total)
            def _():
                pl.semaphore_wait(flood_sem.at[0], 1)
        else:
            flood_finish(at - 1)
        flood_start(at)


    @pl.loop(0, heads)
    def _(head):
        score_grads, query_part, key_part, value_part = pair_terms(
            0, head, qg_ref[0, :, columns(head)], qg_ref[1, :, columns(head)],
            stat[pl.ds(head, 1), :], stat[pl.ds(head + heads, 1), :],
        )
        dq_own[head] = query_part
        dk_acc[head] = key_part
        dv_acc[head] = value_part
        upper = iota((rows, rows), 1) >= iota((rows, rows), 0)
        acc_pos[head] = fold_diagonals(jnp.where(upper, score_grads, 0.0))
        lower = jnp.where(upper, 0.0, score_grads)
        tiles = sum(
            lower[at:at + LANES, at:at + LANES] for at in range(0, rows, LANES)
        )
        acc_neg[head] = fold_diagonals(tiles)
        acc_const[head] = jnp.zeros(acc_const.shape[1:], jnp.float32)

        @pl.when(relays & (lax.rem(head, 2) == 1))
        def _():
            relay(head // 2)

        for at in range(in_loop):
            @pl.when(head == 2 * at + 1)
            def _():
                flood_step(at)

    detours = heads // 2
    leaves = (place == group - 1) & (me // group == 0) & (me + 2 < total)
    passes = (place == 1) & (me // group == 1)

    def leave_copy(head):
        return pltpu.make_async_remote_copy(
            src_ref=part_out.at[0, head], dst_ref=detour_in.at[head],
            send_sem=part_send.at[0], recv_sem=detour_recv.at[0],
            device_id=device(me + 2), device_id_type=MESH,
        )

    def pass_copy(head):
        return pltpu.make_async_remote_copy(
            src_ref=detour_in.at[head], dst_ref=part_in.at[0, head],
            send_sem=detour_send.at[0], recv_sem=part_recv.at[head],
            device_id=device(me - 1), device_id_type=MESH,
        )

    def start_parts(first, last):
        @pl.loop(first, last)
        def _(head):
            detour = leaves & (head < detours)

            @pl.when(detour)
            def _():
                leave_copy(head).start()

            @pl.when(~detour)
            def _():
                part_copy(1, head).start()

    for at in range(in_loop, steps):
        flood_step(at)

    for lag in (2, 1):
        @pl.when(me + lag < total)
        def _():
            stat_copy(lag).wait_recv()

    @pl.loop(0, heads)
    def _(head):
        @pl.when(relays & (head < heads - heads // 2))
        def _():
            relay(head + heads // 2)

        for lag in (2, 1):
            @pl.when(me + lag < total)
            def _():
                @pl.when((lag == 1) | ~relays)
                def _():
                    qg_copy(lag, head).wait_recv()

                score_grads, query_part, key_part, value_part = pair_terms(
                    lag, head, qg_in[lag - 1, head, 0], qg_in[lag - 1, head, 1],
                    stat_in[lag - 1, pl.ds(head, 1), :],
                    stat_in[lag - 1, pl.ds(head + heads, 1), :],
                )
                part_out[lag - 1, head] = query_part.astype(jnp.bfloat16)
                if lag == 2:
                    part_copy(2, head).start()
                dk_acc[head] += key_part
                dv_acc[head] += value_part
                if lag == 1:
                    upper = iota((rows, rows), 1) >= iota((rows, rows), 0)
                    acc_const[head] += fold_rows(jnp.where(upper, score_grads, 0.0))
                    acc_pos[head] += fold_diagonals(jnp.where(upper, 0.0, score_grads))
                else:
                    acc_const[head] += fold_rows(score_grads)

        @pl.when((me + 1 < total) & inside & (head == heads - 2))
        def _():
            start_parts(0, heads - held)

        dk_ref[:, columns(head)] = (dk_acc[head] * inv_root).astype(dk_ref.dtype)
        dv_ref[:, columns(head)] = dv_acc[head].astype(dv_ref.dtype)
        near = jnp.sum(sublane_turn(acc_pos[head], -1), axis=0, keepdims=True)
        before = jnp.sum(sublane_turn(acc_neg[head], -1), axis=0, keepdims=True)
        far = jnp.sum(jnp.sum(acc_const[head], axis=0, keepdims=True), axis=1, keepdims=True)
        tail = jnp.broadcast_to(far, (1, table_width - rows))
        tail = jnp.where(iota(tail.shape, 1) == 0, tail, 0.0)
        here = iota(tab.shape, 0) == head
        tab[...] = jnp.where(here, jnp.concatenate([near, tail], axis=1), tab[...])
        neg[...] = jnp.where(iota(neg.shape, 0) == head, before, neg[...])

    spread = jnp.concatenate(
        [neg[...], jnp.zeros((heads, table_width - LANES), jnp.float32)], axis=1
    )
    running = turn(tab[...], SEG_LEN - 1) + turn(spread, -(LANES - (SEG_LEN - 1)))

    def tab_copy(at, place, peer_place):
        stage = stages[at]
        return pltpu.make_async_remote_copy(
            src_ref=tab_slots.at[at, place], dst_ref=tab_slots.at[at, place],
            send_sem=tab_send.at[at], recv_sem=tab_recv.at[at],
            device_id=stage_peer(stage, peer_place), device_id_type=MESH,
        )

    def stage_start(at, block):
        place = stage_place(stages[at])
        tab_slots[at, place] = block
        for offset in range(1, stages[at][1]):
            tab_copy(at, place, lax.rem(place + offset, stages[at][1])).start()

    def stage_finish(at):
        factor = stages[at][1]
        peers = tab_slots.at[at, pl.ds(0, factor - 1)]
        whole(peers, tab_send.at[at], tab_recv.at[at]).wait_recv()
        out = tab_slots[at, 0]
        for member in range(1, factor):
            out = out + tab_slots[at, member]
        return out

    if stages:
        stage_start(0, running)

    @pl.when((me + 1 < total) & ~inside)
    def _():
        start_parts(0, heads - held)

    for at in range(len(stages) - 1):
        stage_start(at + 1, stage_finish(at))

    @pl.when(me + 1 < total)
    def _():
        start_parts(heads - held, heads)

    @pl.when(passes)
    def _():
        whole(detour_in, detour_send.at[0], detour_recv.at[0]).wait_recv()

        @pl.loop(0, detours)
        def _(head):
            pass_copy(head).start()

    @pl.when(me >= 2)
    def _():
        whole(part_in.at[1], part_send.at[1], part_recv.at[heads]).wait_recv()

        @pl.loop(0, heads)
        def _(head):
            dq_own[head] += part_in[1, head].astype(jnp.float32)

    @pl.loop(0, heads)
    def _(head):
        @pl.when(me >= 1)
        def _():
            part_copy(1, head).wait_recv()
            dq_own[head] += part_in[0, head].astype(jnp.float32)

        dq_ref[:, columns(head)] = (dq_own[head] * inv_root).astype(dq_ref.dtype)

    if stages:
        running = stage_finish(len(stages) - 1)
    dt_ref[...] = running[:, 0:table_len]

    for lag in (1, 2):
        @pl.when(me >= lag)
        def _():
            stat_copy(lag).wait_send()

        @pl.when(sends[lag])
        def _():
            whole(qg_ref, qg_send.at[lag - 1], qg_recv.at[lag - 1, 0]).wait_send()

        @pl.when(me + lag < total)
        def _():
            whole(part_out.at[lag - 1], part_send.at[lag - 1], part_recv.at[0]).wait_send()

    @pl.when(relays)
    def _():
        whole(qg_in.at[1], relay_send.at[0], qg_recv.at[0, 0]).wait_send()

    @pl.when(passes)
    def _():
        whole(detour_in, detour_send.at[0], detour_recv.at[0]).wait_send()

    for at, (_, factor) in enumerate(stages):
        peers = tab_slots.at[at, pl.ds(0, factor - 1)]
        whole(peers, tab_send.at[at], tab_recv.at[at]).wait_send()


def store_kernel(*refs):
    sources, targets, sem = refs[:4], refs[4:8], refs[8]
    stores = [pltpu.make_async_copy(sources[at], targets[at], sem.at[at]) for at in range(4)]
    for store in stores:
        store.start()
    for store in stores:
        store.wait()


def local(sizes, query_rows, key_rows, value_rows, out_grad, log_totals, out_dot, bias_table):
    rows, features = query_rows.shape
    heads, table_len = bias_table.shape
    head_dim = features // heads
    assert LEFT_SEGS * SEG_LEN == 2 * rows and rows == REL_CLIP
    assert table_len == REL_CLIP + SEG_LEN and head_dim == LANES
    stage_list = axis_stages(sizes[0] * sizes[1])
    stage_count = max(len(stage_list), 1)
    flood_count = len(flood_reaches(stage_list)) + 1
    assert sizes[0] * sizes[1] % 4 == 0
    slot_count = max([factor for _, factor in stage_list] + [1])
    table_width = -(-(table_len + 1) // LANES) * LANES
    f32, bf16 = jnp.float32, jnp.bfloat16
    vmem = pl.BlockSpec(memory_space=pltpu.VMEM)
    dma = pltpu.SemaphoreType.DMA
    wide = pltpu.VMEM((rows, features), bf16)
    results = pl.pallas_call(
        functools.partial(kernel, sizes),
        out_shape=(wide, wide, wide, pltpu.VMEM((heads, table_len), f32)),
        in_specs=[pl.BlockSpec(memory_space=pltpu.HBM)] * 7,
        out_specs=(vmem,) * 4,
        scratch_shapes=[
            pltpu.VMEM((2, rows, features), bf16),
            pltpu.VMEM((2, rows, features), bf16),
            pltpu.VMEM((2 * heads, rows), f32),
            pltpu.VMEM((heads, table_len), f32),
            dma((5,)),
            pltpu.VMEM((2 * heads, rows), f32),
            pltpu.VMEM((2, 2 * heads, rows), f32),
            pltpu.VMEM((2, heads, 2, rows, head_dim), bf16),
            pltpu.VMEM((2, heads, rows, head_dim), bf16),
            pltpu.VMEM((2, heads, rows, head_dim), bf16),
            pltpu.VMEM((heads, rows, head_dim), f32),
            pltpu.VMEM((heads, rows, head_dim), f32),
            pltpu.VMEM((heads, rows, head_dim), f32),
            pltpu.VMEM((2, heads, rows, rows), f32),
            pltpu.VMEM((rows, rows), f32),
            pltpu.VMEM((heads, table_width), f32),
            pltpu.VMEM((heads, LANES), f32),
            pltpu.VMEM((heads, rows), f32),
            pltpu.VMEM((heads, SUBL, rows), f32),
            pltpu.VMEM((heads, SUBL, LANES), f32),
            pltpu.VMEM((heads, SUBL, rows), f32),
            pltpu.VMEM((stage_count, slot_count, heads, table_width), f32),
            dma((2,)), dma((2,)),
            dma((2,)), dma((2, heads)),
            dma((2,)), dma((heads + 1,)),
            dma((stage_count,)), dma((stage_count,)),
            pltpu.SemaphoreType.REGULAR((flood_count,)),
            pltpu.SemaphoreType.REGULAR((1,)), dma((1,)),
            pltpu.VMEM((heads // 2, rows, head_dim), bf16), dma((1,)), dma((1,)),
        ],
        compiler_params=pltpu.CompilerParams(
            collective_id=0, has_side_effects=True, vmem_limit_bytes=40 * 2**20
        ),
        name="band_backward",
    )(*(pltpu.with_memory_space_constraint(x, pltpu.HBM) for x in (query_rows, key_rows, value_rows, out_grad, log_totals.T, out_dot.T, bias_table)))
    return pl.pallas_call(
        store_kernel,
        out_shape=tuple(jax.ShapeDtypeStruct(x.shape, x.dtype) for x in results),
        in_specs=[vmem] * 4,
        out_specs=(pl.BlockSpec(memory_space=pltpu.HBM),) * 4,
        scratch_shapes=[dma((4,))],
        compiler_params=pltpu.CompilerParams(vmem_limit_bytes=2**20),
        name="store",
    )(*results)


def solution(mesh):
    sizes = (mesh.shape["sp"], mesh.shape["tp"])
    by_rows = P(("sp", "tp"), None)
    return jax.shard_map(
        functools.partial(local, sizes),
        mesh=mesh,
        in_specs=(by_rows,) * 6 + (P(),),
        out_specs=(by_rows, by_rows, by_rows, P()),
        check_vma=False,
    )
```

```python
import functools
import math

import jax
import jax.numpy as jnp
from jax import lax
from jax.experimental import pallas as pl
from jax.experimental.pallas import tpu as pltpu
from jax.sharding import PartitionSpec as P

SEG_LEN = 64
LEFT_SEGS = 8
REL_CLIP = 256
LANES = 128
SUBL = 8
MASKED = -1e30
LOG2E = math.log2(math.e)
MESH = pl.DeviceIdType.MESH


def axis_stages(size):
    stages, stride = [], 1
    while size > 1:
        order = (8, 4, 3, 2, 5, 7) if stages else (4, 3, 2, 5, 7)
        factor = next((f for f in order if size % f == 0), size)
        stages.append((stride, factor))
        stride *= factor
        size //= factor
    return stages


def flood_reaches(stages):
    reaches, reach = [], 2
    while reach < max([stride * (factor - 1) for stride, factor in stages] + [0]):
        reaches.append(reach)
        reach *= 2
    return reaches


def iota(shape, axis):
    return lax.broadcasted_iota(jnp.int32, shape, axis)


def turn(x, amount):
    width = x.shape[1]
    return pltpu.roll(x, amount % width, 1)


def fold_diagonals(x):
    rows = x.shape[0]
    while rows > SUBL:
        half = rows // 2
        x = x[:half] + turn(x[half:], -half)
        rows = half
    return x


def fold_rows(x):
    rows = x.shape[0]
    while rows > SUBL:
        half = rows // 2
        x = x[:half] + x[half:]
        rows = half
    return x


def sublane_turn(x, direction):
    subl = iota(x.shape, 0)
    for bit in (1, 2, 4):
        x = jnp.where((subl & bit) != 0, turn(x, direction * bit), x)
    return x


def kernel(
    sizes,
    q_hbm, k_hbm, v_hbm, g_hbm, log_hbm, dot_hbm, table_hbm,
    dq_ref, dk_ref, dv_ref, dt_ref,
    qg_ref, kv_ref, rows_ref, table_ref, load_sem,
    stat, stat_in, qg_in, part_out, part_in, dq_own, dk_acc, dv_acc,
    bias, edge, tab, neg, const, acc_pos, acc_neg, acc_const, tab_slots,
    stat_send, stat_recv, qg_send, qg_recv, part_send, part_recv, tab_send, tab_recv,
    flood_sem, go_sem, relay_send,
):
    sp_size, tp_size = sizes
    total = sp_size * tp_size
    _, rows, features = qg_ref.shape
    heads, table_len = table_ref.shape
    head_dim = features // heads
    inv_root = head_dim ** -0.5
    table_width = tab.shape[1]
    sp, tp = lax.axis_index("sp"), lax.axis_index("tp")
    me = sp * tp_size + tp

    def device(index):
        return (index // tp_size, lax.rem(index, tp_size))

    stages = axis_stages(total)[::-1]

    group = stages[-1][1] if stages else 1
    inside = (lax.rem(me + 1, group) != 0) | (lax.rem((me + 1) // group, 2) == 1)
    sends = [None, (me >= 1) & (lax.rem(me, group) != 0), me >= 2]
    relays = (me + 2 < total) & (lax.rem(me + 2, group) == 0)

    def stage_place(stage):
        stride, factor = stage
        return lax.rem(me // stride, factor)

    def stage_peer(stage, place):
        return device(me + (place - stage_place(stage)) * stage[0])

    def columns(head):
        return pl.ds(pl.multiple_of(head * head_dim, head_dim), head_dim)

    first, others = pl.ds(0, head_dim), pl.ds(head_dim, features - head_dim)
    stat_rows = (pl.ds(0, heads), pl.ds(heads, heads))
    loads = [
        [(q_hbm.at[:, first], qg_ref.at[0, :, first]), (g_hbm.at[:, first], qg_ref.at[1, :, first])],
        [(log_hbm, rows_ref.at[stat_rows[0]]), (dot_hbm, rows_ref.at[stat_rows[1]])],
        [(q_hbm.at[:, others], qg_ref.at[0, :, others]), (g_hbm.at[:, others], qg_ref.at[1, :, others])],
        [(table_hbm, table_ref)],
        [(k_hbm, kv_ref.at[0]), (v_hbm, kv_ref.at[1])],
    ]
    loaded = [qg_ref.at[:, :, first], rows_ref, qg_ref.at[:, :, others], table_ref, kv_ref]

    def load_start(at):
        for source, target in loads[at]:
            pltpu.make_async_copy(source, target, load_sem.at[at]).start()

    def load_wait(at):
        pltpu.make_async_copy(loaded[at], loaded[at], load_sem.at[at]).wait()

    place = lax.rem(me, group)
    held = min(2, heads)
    barrier = pltpu.get_barrier_semaphore()
    for other, valid in (
        (me + 2, (me + 2 < total) & (place != group - 1)),
        (me + 1, me + 1 < total),
        (me - 1, lax.rem(place, 2) == 1),
    ):
        @pl.when(valid)
        def _():
            pl.semaphore_signal(barrier, inc=1, device_id=device(other), device_id_type=MESH)

    awaited = (me >= 1, (me >= 2) & (place != 1), (lax.rem(place, 2) == 0) & (me + 1 < total))
    count = sum(jnp.where(valid, 1, 0) for valid in awaited)

    for at in range(len(loads)):
        load_start(at)
    pl.semaphore_wait(barrier, count)

    def stat_copy(lag):
        return pltpu.make_async_remote_copy(
            src_ref=stat, dst_ref=stat_in.at[lag - 1],
            send_sem=stat_send.at[lag - 1], recv_sem=stat_recv.at[lag - 1],
            device_id=device(me - lag), device_id_type=MESH,
        )

    def qg_copy(lag, head):
        return pltpu.make_async_remote_copy(
            src_ref=qg_ref.at[:, :, columns(head)], dst_ref=qg_in.at[lag - 1, head],
            send_sem=qg_send.at[lag - 1], recv_sem=qg_recv.at[lag - 1, head],
            device_id=device(me - lag), device_id_type=MESH,
        )

    def relay_copy(head):
        return pltpu.make_async_remote_copy(
            src_ref=qg_in.at[1, head], dst_ref=qg_in.at[0, head],
            send_sem=relay_send.at[0], recv_sem=qg_recv.at[0, head],
            device_id=device(me + 1), device_id_type=MESH,
        )

    def relay(head):
        qg_copy(2, head).wait_recv()
        relay_copy(head).start()

    def part_copy(lag, head):
        return pltpu.make_async_remote_copy(
            src_ref=part_out.at[lag - 1, head], dst_ref=part_in.at[lag - 1, head],
            send_sem=part_send.at[lag - 1],
            recv_sem=part_recv.at[jnp.maximum(head - (heads - held), -1) + 2 if lag == 1 else 0],
            device_id=device(me + lag), device_id_type=MESH,
        )

    def whole(ref, send_sem, recv_sem):
        return pltpu.make_async_remote_copy(
            src_ref=ref, dst_ref=ref, send_sem=send_sem, recv_sem=recv_sem,
            device_id=device(me), device_id_type=MESH,
        )

    for which, source in enumerate((q_hbm, g_hbm)):
        @pl.when(sends[1])
        def _():
            pltpu.make_async_remote_copy(
                src_ref=source.at[:, first], dst_ref=qg_in.at[0, 0, which],
                send_sem=qg_send.at[0], recv_sem=qg_recv.at[0, 0],
                device_id=device(me - 1), device_id_type=MESH,
            ).start()

    @pl.when((place == 0) & (me >= 1))
    def _():
        pl.semaphore_signal(go_sem.at[0], inc=1, device_id=device(me + 1), device_id_type=MESH)

    @pl.when(sends[2] & (place != 1))
    def _():
        load_wait(0)
        qg_copy(2, 0).start()

    @pl.when(~(sends[2] & (place != 1)))
    def _():
        load_wait(0)

    load_wait(1)
    stat[0:heads, :] = rows_ref[0:heads, :] * LOG2E
    stat[heads:, :] = rows_ref[heads:, :]

    @pl.when(me >= 1)
    def _():
        stat_copy(1).start()

    @pl.when(sends[2] & (place != 1))
    def _():
        stat_copy(2).start()

    load_wait(2)

    @pl.loop(1, heads)
    def _(head):
        @pl.when(sends[1])
        def _():
            qg_copy(1, head).start()

        @pl.when(sends[2] & (place != 1))
        def _():
            qg_copy(2, head).start()

    @pl.when(sends[2])
    def _():
        @pl.when(place == 1)
        def _():
            pl.semaphore_wait(go_sem.at[0], 1)
            stat_copy(2).start()

            @pl.loop(0, heads)
            def _(head):
                qg_copy(2, head).start()

        pl.semaphore_signal(flood_sem.at[0], inc=1, device_id=device(me - 2), device_id_type=MESH)

    reaches = flood_reaches(stages)

    def flood_others(at):
        others = (me + reaches[at], me - reaches[at])
        return [(other, (other >= 0) & (other < total)) for other in others]

    def flood_start(at):
        if at < len(reaches):
            for other, valid in flood_others(at):
                @pl.when(valid)
                def _():
                    pl.semaphore_signal(
                        flood_sem.at[at + 1], inc=1, device_id=device(other), device_id_type=MESH
                    )

    def flood_finish(at):
        if at < len(reaches):
            valid = [valid for _, valid in flood_others(at)]

            @pl.when(valid[0] | valid[1])
            def _():
                pl.semaphore_wait(
                    flood_sem.at[at + 1], sum(jnp.where(each, 1, 0) for each in valid)
                )

    load_wait(3)
    tab[...] = jnp.zeros_like(tab)
    tab[:, 0:table_len] = table_ref[...] * LOG2E
    padded = tab[...]
    from_zero = turn(padded, 1 - SEG_LEN)
    neg[...] = turn(padded, LANES - (SEG_LEN - 1))[:, 0:LANES]
    const[...] = jnp.broadcast_to(from_zero[:, rows:rows + 1], const.shape)
    tab[...] = from_zero
    key_at, query_at = iota((rows, rows), 0), iota((rows, rows), 1)
    edge[...] = jnp.where(query_at // SEG_LEN <= key_at // SEG_LEN, 0.0, MASKED)

    @pl.loop(0, heads)
    def _(head):
        row = jnp.broadcast_to(tab[pl.ds(head, 1), 0:rows], (SUBL, rows))
        near = sublane_turn(row, 1)
        row = jnp.broadcast_to(neg[pl.ds(head, 1), :], (SUBL, LANES))
        before = sublane_turn(row, 1)
        have = SUBL
        while have < rows:
            near = jnp.concatenate([near, turn(near, have)], axis=0)
            if have < LANES:
                before = jnp.concatenate([before, turn(before, have)], axis=0)
            have *= 2
        far = const[pl.ds(head, 1), :]
        upper = iota((rows, rows), 1) >= iota((rows, rows), 0)
        bias[1, head] = jnp.where(upper, far, near)
        segs_ok = iota((rows, rows), 1) // SEG_LEN >= iota((rows, rows), 0) // SEG_LEN
        wide = jnp.concatenate([before] * (rows // LANES), axis=1)
        tall = jnp.concatenate([wide] * (rows // LANES), axis=0)
        bias[0, head] = jnp.where(upper, near, jnp.where(segs_ok, tall, MASKED))

    def pair_terms(lag, head, queries, grads, log_row, dot_row):
        keys, values = kv_ref[0, :, columns(head)], kv_ref[1, :, columns(head)]
        across = (((1,), (1,)), ((), ()))
        scores = lax.dot_general(keys, queries, across, preferred_element_type=jnp.float32)
        if lag < 2:
            shift = bias[lag, head] - log_row
        else:
            shift = edge[...] + (const[pl.ds(head, 1), :] - log_row)
        weights = jnp.exp2(scores * (inv_root * LOG2E) + shift)
        weight_grads = lax.dot_general(values, grads, across, preferred_element_type=jnp.float32)
        score_grads = weights * (weight_grads - dot_row)
        score_grads_b = score_grads.astype(jnp.bfloat16)
        value_part = jnp.dot(
            weights.astype(jnp.bfloat16), grads, preferred_element_type=jnp.float32
        )
        key_part = jnp.dot(score_grads_b, queries, preferred_element_type=jnp.float32)
        query_part = lax.dot_general(
            score_grads_b, keys, (((0,), (0,)), ((), ())), preferred_element_type=jnp.float32
        )
        return score_grads, query_part, key_part, value_part

    load_wait(4)
    steps = len(reaches) + 1 if stages else 0
    in_loop = min(steps, heads // 2)

    def flood_step(at):
        if at == 0:
            @pl.when(me + 2 < total)
            def _():
                pl.semaphore_wait(flood_sem.at[0], 1)
        else:
            flood_finish(at - 1)
        flood_start(at)


    @pl.loop(0, heads)
    def _(head):
        score_grads, query_part, key_part, value_part = pair_terms(
            0, head, qg_ref[0, :, columns(head)], qg_ref[1, :, columns(head)],
            stat[pl.ds(head, 1), :], stat[pl.ds(head + heads, 1), :],
        )
        dq_own[head] = query_part
        dk_acc[head] = key_part
        dv_acc[head] = value_part
        upper = iota((rows, rows), 1) >= iota((rows, rows), 0)
        acc_pos[head] = fold_diagonals(jnp.where(upper, score_grads, 0.0))
        lower = jnp.where(upper, 0.0, score_grads)
        tiles = sum(
            lower[at:at + LANES, at:at + LANES] for at in range(0, rows, LANES)
        )
        acc_neg[head] = fold_diagonals(tiles)
        acc_const[head] = jnp.zeros(acc_const.shape[1:], jnp.float32)

        @pl.when(relays & (lax.rem(head, 2) == 1))
        def _():
            relay(head // 2)

        for at in range(in_loop):
            @pl.when(head == 2 * at + 1)
            def _():
                flood_step(at)

    def start_parts(first, last):
        @pl.loop(first, last)
        def _(head):
            part_copy(1, head).start()

    for at in range(in_loop, steps):
        flood_step(at)

    for lag in (2, 1):
        @pl.when(me + lag < total)
        def _():
            stat_copy(lag).wait_recv()

    @pl.loop(0, heads)
    def _(head):
        @pl.when(relays & (head < heads - heads // 2))
        def _():
            relay(head + heads // 2)

        for lag in (2, 1):
            @pl.when(me + lag < total)
            def _():
                @pl.when((lag == 1) | ~relays)
                def _():
                    qg_copy(lag, head).wait_recv()

                score_grads, query_part, key_part, value_part = pair_terms(
                    lag, head, qg_in[lag - 1, head, 0], qg_in[lag - 1, head, 1],
                    stat_in[lag - 1, pl.ds(head, 1), :],
                    stat_in[lag - 1, pl.ds(head + heads, 1), :],
                )
                part_out[lag - 1, head] = query_part.astype(jnp.bfloat16)
                if lag == 2:
                    part_copy(2, head).start()
                dk_acc[head] += key_part
                dv_acc[head] += value_part
                if lag == 1:
                    upper = iota((rows, rows), 1) >= iota((rows, rows), 0)
                    acc_const[head] += fold_rows(jnp.where(upper, score_grads, 0.0))
                    acc_pos[head] += fold_diagonals(jnp.where(upper, 0.0, score_grads))
                else:
                    acc_const[head] += fold_rows(score_grads)

        @pl.when((me + 1 < total) & inside & (head == heads - 2))
        def _():
            start_parts(0, heads - held)

        dk_ref[:, columns(head)] = (dk_acc[head] * inv_root).astype(dk_ref.dtype)
        dv_ref[:, columns(head)] = dv_acc[head].astype(dv_ref.dtype)
        near = jnp.sum(sublane_turn(acc_pos[head], -1), axis=0, keepdims=True)
        before = jnp.sum(sublane_turn(acc_neg[head], -1), axis=0, keepdims=True)
        far = jnp.sum(jnp.sum(acc_const[head], axis=0, keepdims=True), axis=1, keepdims=True)
        tail = jnp.broadcast_to(far, (1, table_width - rows))
        tail = jnp.where(iota(tail.shape, 1) == 0, tail, 0.0)
        here = iota(tab.shape, 0) == head
        tab[...] = jnp.where(here, jnp.concatenate([near, tail], axis=1), tab[...])
        neg[...] = jnp.where(iota(neg.shape, 0) == head, before, neg[...])

    spread = jnp.concatenate(
        [neg[...], jnp.zeros((heads, table_width - LANES), jnp.float32)], axis=1
    )
    running = turn(tab[...], SEG_LEN - 1) + turn(spread, -(LANES - (SEG_LEN - 1)))

    def tab_copy(at, place, peer_place):
        stage = stages[at]
        return pltpu.make_async_remote_copy(
            src_ref=tab_slots.at[at, place], dst_ref=tab_slots.at[at, place],
            send_sem=tab_send.at[at], recv_sem=tab_recv.at[at],
            device_id=stage_peer(stage, peer_place), device_id_type=MESH,
        )

    def stage_start(at, block):
        place = stage_place(stages[at])
        tab_slots[at, place] = block
        for offset in range(1, stages[at][1]):
            tab_copy(at, place, lax.rem(place + offset, stages[at][1])).start()

    def stage_finish(at):
        factor = stages[at][1]
        peers = tab_slots.at[at, pl.ds(0, factor - 1)]
        whole(peers, tab_send.at[at], tab_recv.at[at]).wait_recv()
        out = tab_slots[at, 0]
        for member in range(1, factor):
            out = out + tab_slots[at, member]
        return out

    if stages:
        stage_start(0, running)

    @pl.when((me + 1 < total) & ~inside)
    def _():
        start_parts(0, heads - held)

    for at in range(len(stages) - 1):
        stage_start(at + 1, stage_finish(at))

    @pl.when(me + 1 < total)
    def _():
        start_parts(heads - held, heads)

    @pl.when(me >= 2)
    def _():
        whole(part_in.at[1], part_send.at[1], part_recv.at[0]).wait_recv()

        @pl.loop(0, heads)
        def _(head):
            dq_own[head] += part_in[1, head].astype(jnp.float32)

    @pl.when(me >= 1)
    def _():
        early = part_in.at[0, pl.ds(0, heads - held)]
        whole(early, part_send.at[0], part_recv.at[1]).wait_recv()

    @pl.loop(0, heads)
    def _(head):
        @pl.when(me >= 1)
        def _():
            @pl.when(head >= heads - held)
            def _():
                part_copy(1, head).wait_recv()

            dq_own[head] += part_in[0, head].astype(jnp.float32)

        dq_ref[:, columns(head)] = (dq_own[head] * inv_root).astype(dq_ref.dtype)

    if stages:
        running = stage_finish(len(stages) - 1)
    dt_ref[...] = running[:, 0:table_len]

    for lag in (1, 2):
        @pl.when(me >= lag)
        def _():
            stat_copy(lag).wait_send()

        @pl.when(sends[lag])
        def _():
            whole(qg_ref, qg_send.at[lag - 1], qg_recv.at[lag - 1, 0]).wait_send()

        @pl.when(me + lag < total)
        def _():
            whole(part_out.at[lag - 1], part_send.at[lag - 1], part_recv.at[0]).wait_send()

    @pl.when(relays)
    def _():
        whole(qg_in.at[1], relay_send.at[0], qg_recv.at[0, 0]).wait_send()

    for at, (_, factor) in enumerate(stages):
        peers = tab_slots.at[at, pl.ds(0, factor - 1)]
        whole(peers, tab_send.at[at], tab_recv.at[at]).wait_send()


def store_kernel(*refs):
    sources, targets, sem = refs[:4], refs[4:8], refs[8]
    stores = [pltpu.make_async_copy(sources[at], targets[at], sem.at[at]) for at in range(4)]
    for store in stores:
        store.start()
    for store in stores:
        store.wait()


def local(sizes, query_rows, key_rows, value_rows, out_grad, log_totals, out_dot, bias_table):
    rows, features = query_rows.shape
    heads, table_len = bias_table.shape
    head_dim = features // heads
    assert LEFT_SEGS * SEG_LEN == 2 * rows and rows == REL_CLIP
    assert table_len == REL_CLIP + SEG_LEN and head_dim == LANES
    stage_list = axis_stages(sizes[0] * sizes[1])
    stage_count = max(len(stage_list), 1)
    flood_count = len(flood_reaches(stage_list)) + 1
    assert sizes[0] * sizes[1] % 4 == 0
    slot_count = max([factor for _, factor in stage_list] + [1])
    table_width = -(-(table_len + 1) // LANES) * LANES
    f32, bf16 = jnp.float32, jnp.bfloat16
    vmem = pl.BlockSpec(memory_space=pltpu.VMEM)
    dma = pltpu.SemaphoreType.DMA
    wide = pltpu.VMEM((rows, features), bf16)
    results = pl.pallas_call(
        functools.partial(kernel, sizes),
        out_shape=(wide, wide, wide, pltpu.VMEM((heads, table_len), f32)),
        in_specs=[pl.BlockSpec(memory_space=pltpu.HBM)] * 7,
        out_specs=(vmem,) * 4,
        scratch_shapes=[
            pltpu.VMEM((2, rows, features), bf16),
            pltpu.VMEM((2, rows, features), bf16),
            pltpu.VMEM((2 * heads, rows), f32),
            pltpu.VMEM((heads, table_len), f32),
            dma((5,)),
            pltpu.VMEM((2 * heads, rows), f32),
            pltpu.VMEM((2, 2 * heads, rows), f32),
            pltpu.VMEM((2, heads, 2, rows, head_dim), bf16),
            pltpu.VMEM((2, heads, rows, head_dim), bf16),
            pltpu.VMEM((2, heads, rows, head_dim), bf16),
            pltpu.VMEM((heads, rows, head_dim), f32),
            pltpu.VMEM((heads, rows, head_dim), f32),
            pltpu.VMEM((heads, rows, head_dim), f32),
            pltpu.VMEM((2, heads, rows, rows), f32),
            pltpu.VMEM((rows, rows), f32),
            pltpu.VMEM((heads, table_width), f32),
            pltpu.VMEM((heads, LANES), f32),
            pltpu.VMEM((heads, rows), f32),
            pltpu.VMEM((heads, SUBL, rows), f32),
            pltpu.VMEM((heads, SUBL, LANES), f32),
            pltpu.VMEM((heads, SUBL, rows), f32),
            pltpu.VMEM((stage_count, slot_count, heads, table_width), f32),
            dma((2,)), dma((2,)),
            dma((2,)), dma((2, heads)),
            dma((2,)), dma((4,)),
            dma((stage_count,)), dma((stage_count,)),
            pltpu.SemaphoreType.REGULAR((flood_count,)),
            pltpu.SemaphoreType.REGULAR((1,)), dma((1,)),
        ],
        compiler_params=pltpu.CompilerParams(
            collective_id=0, has_side_effects=True, vmem_limit_bytes=40 * 2**20
        ),
        name="band_backward",
    )(*(pltpu.with_memory_space_constraint(x, pltpu.HBM) for x in (query_rows, key_rows, value_rows, out_grad, log_totals.T, out_dot.T, bias_table)))
    return pl.pallas_call(
        store_kernel,
        out_shape=tuple(jax.ShapeDtypeStruct(x.shape, x.dtype) for x in results),
        in_specs=[vmem] * 4,
        out_specs=(pl.BlockSpec(memory_space=pltpu.HBM),) * 4,
        scratch_shapes=[dma((4,))],
        compiler_params=pltpu.CompilerParams(vmem_limit_bytes=2**20),
        name="store",
    )(*results)


def solution(mesh):
    sizes = (mesh.shape["sp"], mesh.shape["tp"])
    by_rows = P(("sp", "tp"), None)
    return jax.shard_map(
        functools.partial(local, sizes),
        mesh=mesh,
        in_specs=(by_rows,) * 6 + (P(),),
        out_specs=(by_rows, by_rows, by_rows, P()),
        check_vma=False,
    )
```
